128 devices in a mesh: grp: 4 (over y, x), ep: 32 (over z, core).
Axes of the slice: x: 2, y: 2, z: 16, core: 2. Of those that a mesh axis runs over, the one named last changes fastest.
The devices are a block of a 8x8x16 slice.
Arguments:
- tokens: bfloat16 [1024, 2048], P(('grp', 'ep')), parts along dimension 0, may hold values from -6 to 6
- state: float32 [1024, 8, 64, 128], P(('grp', 'ep')), parts along dimension 0, may hold values from -6 to 6
- g_mix: float32 [2048], replicated, may hold values from 0.1 to 1.9
- w_query: bfloat16 [2048, 512], P('ep'), may hold values from -0.125 to 0.125
- w_key: bfloat16 [2048, 512], P('ep'), may hold values from -0.125 to 0.125
- w_value: bfloat16 [2048, 1024], P('ep'), may hold values from -0.125 to 0.125
- w_decay_down: bfloat16 [2048, 32], replicated, may hold values from -0.125 to 0.125
- w_decay_up: bfloat16 [32, 512], replicated, may hold values from -1 to 1
- decay_bias: float32 [512], replicated, may hold values from -6 to 2
- g_head: float32 [128], replicated, may hold values from 0.1 to 1.9
- w_out: bfloat16 [1024, 2048], replicated, may hold values from -0.1875 to 0.1875
- g_ffn: float32 [2048], replicated, may hold values from 0.1 to 1.9
- routes: int32 [1024, 4], P(('grp', 'ep')), parts along dimension 0, may hold values from 0 to 31, all different within a row; in each aligned block of 8 rows (0 to 7, 8 to 15, ...) at most 2 rows name the same one
- route_scores: float32 [1024, 4], P(('grp', 'ep')), parts along dimension 0, may hold values from -9 to 320
- w_gate_in: bfloat16 [32, 2048, 1024], P('ep'), may hold values from -0.375 to 0.375
- w_lin_in: bfloat16 [32, 2048, 1024], P('ep'), may hold values from -0.375 to 0.375
- w_down: bfloat16 [32, 1024, 2048], P('ep'), may hold values from -0.046875 to 0.046875
Outputs:
- output: bfloat16 [1024, 2048], P(('grp', 'ep')), parts along dimension 0
- new_state: float32 [1024, 8, 64, 128], P(('grp', 'ep')), parts along dimension 0
The draws below stay inside these ranges and needn't reach their ends.
There are 4 independent parts, one for each index of `grp`. The reference program is written for one: setup_inputs(seed, part) draws one part's arguments, and reference() takes and returns one part's arrays. A program takes and returns all parts, laid end to end along the dimension named above; an argument that names none is the same for every part. Nothing has to cross between parts.
Inputs may be any that keep to these rules, and one draw needn't show every extreme that they name: `routes`: each row names 4 different experts; the rows of one device name no expert more than 2 times, a bound that some block reaches.
All inputs are finite; a program needn't handle non-finite values.
Results may differ from the reference program's by a relative error of at most 0.014.
Values may be sent and summed in bfloat16 or wider, within the bound.
A program may use at most 128 MiB of HBM per device.

```python
import math
import jax
import jax.numpy as jnp
import numpy as np
from jax import lax

D = 2048
HEADS = 8
DK = 64
DV = 128
RANK = 32
FF = 1024
EXPERTS = 32
TOPK = 4
CAP = 2
SEQ_DEV = 8
QK = 512
VW = 1024
TOKENS = 256


def draw_route_scores(key, part):
    base_key = jax.random.fold_in(jax.random.fold_in(key, 11), 0)
    scores = jnp.clip(1.5 * jax.random.normal(base_key, (TOKENS, TOPK), jnp.float32), -9.0, 9.0)
    return scores


def steps_of(rng, extent, shards, low, high):
    def one(dim, parts):
        draws = jax.random.uniform(jax.random.fold_in(jax.random.fold_in(rng, 6), dim), (parts,), jnp.float32, low / len(shards), high / len(shards))
        return jnp.repeat(jnp.exp(draws), extent[dim] // parts).reshape((-1,) + (1,) * (len(extent) - dim - 1))

    loudness = one(*shards[0])
    for cut in shards[1:]:
        loudness = loudness * one(*cut)
    return loudness


def assign_block(stream_key, own, number, rows, count, top, most, slope):
    ranking = jax.random.permutation(stream_key, count)
    crowded, ordinary = portions_of(count, rows * top, most, slope, True), portions_of(count, rows * top, most, slope, False)
    places = jnp.arange(count)

    def named(lengths, turn):
        used = int((lengths > 0).sum())
        fixed = max(1, used // 4)
        shifted = fixed + (places - fixed + turn * (used - fixed)) % max(1, count - fixed)
        return jnp.zeros((count,), jnp.int32).at[ranking[jnp.where(places < fixed, places, shifted)]].set(jnp.asarray(lengths, jnp.int32))

    lengths = jnp.where(number % 4 == 0, named(crowded, number // 4), named(ordinary, number - number // 4 - 1))
    mixed = jax.random.permutation(jax.random.fold_in(own, 3), count)
    donor, sink = mixed[0:count // 2 * 2:2], mixed[1:count // 2 * 2:2]
    room = jnp.minimum(lengths[donor] - 1, most - lengths[sink]) // 2
    room = jnp.where((donor == ranking[0]) | (sink == ranking[0]) | (lengths[sink] == 0), 0, jnp.maximum(room, 0))
    shifted = jax.random.randint(jax.random.fold_in(own, 4), (count // 2,), 0, 1 << 20) % (room + 1)
    lengths = lengths.at[donor].add(-shifted).at[sink].add(shifted)
    items = jnp.searchsorted(jnp.cumsum(lengths), jnp.arange(rows * top), side="right").astype(jnp.int32)
    table = items.reshape(top, rows).T
    table = table[jax.random.permutation(jax.random.fold_in(own, 1), rows)]
    turn = jax.random.randint(jax.random.fold_in(own, 2), (rows, 1), 0, top)
    return jnp.take_along_axis(table, (jnp.arange(top)[None, :] + turn) % top, axis=1)


def portions_of(number_of, total, limit, slope, full):
    loads = [(1 << 20) // math.isqrt(rank ** slope) + 1 for rank in range(1, number_of + 1)]
    largest = limit if full else min(limit, max(-(-total // number_of), total * loads[0] // sum(loads)))
    least = 1 if total - largest >= number_of - 1 else 0
    holding, spare = [largest] + [least] * (number_of - 1), total - largest - least * (number_of - 1)
    while spare > 0:
        movable = [i for i in range(1, number_of) if holding[i] < largest] or [i for i in range(1, number_of) if holding[i] < limit]
        mass, left = sum([loads[i] for i in movable]), spare
        for i in movable:
            addition = min(limit - holding[i], max(1, left * loads[i] // mass), spare)
            holding[i] = holding[i] + addition
            spare = spare - addition
    return np.array(holding)


def centred(own_key, dims, scale, most, pieces=(), held_as=jnp.bfloat16):
    level = steps_of(own_key, dims, pieces, -0.22, 0.18) if pieces else 1.0
    entries = jax.random.normal(own_key, dims, jnp.float32) * scale * level
    return jnp.minimum(jnp.maximum(entries, -most), most).astype(held_as)


def setup_inputs(seed: int = 0, part: int = 0) -> dict:
    key_list = jax.random.split(jax.random.key(seed), 18)
    part_splits = jax.random.split(jax.random.fold_in(key_list[17], part), 18)
    tokens = centred(part_splits[0], (TOKENS, D), 1.0, 6.0, ((0, 32),))
    state = centred(part_splits[1], (TOKENS, HEADS, DK, DV), 1.0, 6.0, ((0, 32),), jnp.float32)
    g_mix = jnp.clip(1.0 + 0.18 * jax.random.normal(key_list[2], (D,), jnp.float32), 0.1, 1.9)
    w_query = centred(key_list[3], (D, QK), D ** -0.5, 0.125, ((0, 32),))
    w_key = centred(key_list[4], (D, QK), D ** -0.5, 0.125, ((0, 32),))
    w_value = centred(key_list[5], (D, VW), D ** -0.5, 0.125, ((0, 32),))
    w_decay_down = centred(key_list[6], (D, RANK), D ** -0.5, 0.125)
    w_decay_up = centred(key_list[7], (RANK, QK), RANK ** -0.5, 1.0)
    decay_bias = jnp.clip(jax.random.uniform(key_list[8], (QK,), jnp.float32, -6.0, 2.0), -6.0, 2.0)
    g_head = jnp.clip(1.0 + 0.18 * jax.random.normal(key_list[9], (DV,), jnp.float32), 0.1, 1.9)
    w_out = centred(key_list[10], (VW, D), VW ** -0.5, 0.1875)
    g_ffn = jnp.clip(1.0 + 0.18 * jax.random.normal(key_list[11], (D,), jnp.float32), 0.1, 1.9)
    routes_keys = jax.random.split(jax.random.fold_in(part_splits[12], 1), TOKENS // SEQ_DEV)
    routes_turns = jax.random.permutation(jax.random.fold_in(part_splits[12], 3), TOKENS // SEQ_DEV)
    routes = jax.vmap(lambda own, number: assign_block(jax.random.fold_in(part_splits[12], 2), own, number, SEQ_DEV, EXPERTS, TOPK, CAP, 2))(routes_keys, routes_turns).reshape((TOKENS, TOPK))
    route_scores = draw_route_scores(jax.random.fold_in(jax.random.fold_in(key_list[17], part), 71), part)
    w_gate_in = centred(key_list[14], (EXPERTS, D, FF), (D // 8) ** -0.5, 0.375, ((0, 32),))
    w_lin_in = centred(key_list[15], (EXPERTS, D, FF), (D // 8) ** -0.5, 0.375, ((0, 32),))
    w_down = centred(key_list[16], (EXPERTS, FF, D), (FF * 16) ** -0.5, 0.046875, ((0, 32),))
    return {"tokens": tokens, "state": state, "g_mix": g_mix, "w_query": w_query, "w_key": w_key, "w_value": w_value, "w_decay_down": w_decay_down, "w_decay_up": w_decay_up, "decay_bias": decay_bias, "g_head": g_head, "w_out": w_out, "g_ffn": g_ffn, "routes": routes, "route_scores": route_scores, "w_gate_in": w_gate_in, "w_lin_in": w_lin_in, "w_down": w_down}


EPS = 1e-06
TAU = 16.0
ALPHA = 1.702
LIMIT = 7.0

def rms_scale(values, gain):
    return values * lax.rsqrt(lax.optimization_barrier(jnp.mean(values * values, axis=-1, keepdims=True)) + EPS) * gain

def expert_apply(fed, gate_weight, lin_weight, down_weight):
    gate_pre = jnp.minimum(jnp.dot(fed, gate_weight, preferred_element_type=jnp.float32), LIMIT)
    lin_pre = jnp.clip(jnp.dot(fed, lin_weight, preferred_element_type=jnp.float32), -LIMIT, LIMIT)
    hidden = (gate_pre * jax.nn.sigmoid(ALPHA * gate_pre) * (lin_pre + 1.0)).astype(jnp.bfloat16)
    return jnp.dot(hidden, down_weight, preferred_element_type=jnp.float32).astype(jnp.bfloat16)

def reference(tokens, state, g_mix, w_query, w_key, w_value, w_decay_down, w_decay_up, decay_bias, g_head, w_out, g_ffn, routes, route_scores, w_gate_in, w_lin_in, w_down):
    seq_rows = tokens.shape[0]
    normed = rms_scale(tokens.astype(jnp.float32), g_mix).astype(jnp.bfloat16)
    queries = jnp.dot(normed, w_query, preferred_element_type=jnp.float32).reshape(seq_rows, HEADS, DK) * DK ** (-0.5)
    key_rows = jnp.dot(normed, w_key, preferred_element_type=jnp.float32).reshape(seq_rows, HEADS, DK)
    value_rows = jnp.dot(normed, w_value, preferred_element_type=jnp.float32).reshape(seq_rows, HEADS, DV)
    low_rank = jnp.dot(normed, w_decay_down, preferred_element_type=jnp.float32).astype(jnp.bfloat16)
    log_decay = jax.nn.log_sigmoid(jnp.dot(low_rank, w_decay_up, preferred_element_type=jnp.float32) + decay_bias) / TAU
    log_decay = log_decay.reshape(seq_rows, HEADS, DK)
    new_state = jnp.exp(log_decay)[..., None] * state + key_rows[..., None] * value_rows[:, :, None, :]
    attended = jnp.einsum('bhk,bhkv->bhv', queries, new_state, precision=lax.Precision.HIGHEST)
    headed = rms_scale(attended, g_head).astype(jnp.bfloat16).reshape(seq_rows, HEADS * DV)
    residual = (tokens.astype(jnp.float32) + jnp.dot(headed, w_out, preferred_element_type=jnp.float32)).astype(jnp.bfloat16)
    fed = rms_scale(residual.astype(jnp.float32), g_ffn).astype(jnp.bfloat16)
    weights = jax.nn.softmax(route_scores, axis=-1)

    def expert_step(expert_index, running):
        chosen = lax.optimization_barrier(jnp.sum(jnp.where(routes == expert_index, weights, jnp.zeros_like(weights)), axis=1))
        expert_out = expert_apply(fed, w_gate_in[expert_index], w_lin_in[expert_index], w_down[expert_index])
        return running + chosen[:, None] * expert_out.astype(jnp.float32)
    expert_sum = lax.fori_loop(0, EXPERTS, expert_step, jnp.zeros((seq_rows, D), jnp.float32))
    output = (residual.astype(jnp.float32) + expert_sum).astype(jnp.bfloat16)
    return (output, new_state)
```

```python
import functools

import jax
import jax.numpy as jnp
from jax import lax
from jax.experimental import pallas as pl
from jax.experimental.pallas import tpu as pltpu
from jax.sharding import PartitionSpec as P

MESH = pl.DeviceIdType.MESH
F32 = jnp.float32
BF16 = jnp.bfloat16

HEADS = 8
DK = 64
DV = 128
CAP = 2
EPS = 1e-06
TAU = 16.0
ALPHA = 1.702
LIMIT = 7.0

OFFSETS = (0, 3, -3, 6, -6, 8)
SEND_ORDER = (5, 3, 4, 1, 2, 0)


def rms(values, gain):
    return values * lax.rsqrt(jnp.mean(values * values, axis=-1, keepdims=True) + EPS) * gain


def dot(a, b, dims=None, precision=None):
    dims = dims or (((1,), (0,)), ((), ()))
    return lax.dot_general(a, b, dims, precision=precision, preferred_element_type=F32)


def iota(shape, dim):
    return lax.broadcasted_iota(jnp.int32, shape, dim)


def kernel(
    ep,
    tokens,
    g_mix,
    w_dd,
    w_du,
    d_bias,
    g_head,
    g_ffn,
    routes,
    scores,
    state,
    w_q,
    w_k,
    w_v,
    w_out,
    w_gate,
    w_lin,
    w_down,
    out,
    key_out,
    value_out,
    decay_out,
    own_w,
    st,
    wo,
    wg,
    wl,
    wd,
    xs,
    xbuf,
    wbuf,
    psend,
    rbuf,
    dsend,
    drecv,
    rsend,
    rrecv,
    xin,
    hid,
    eo,
    perm,
    perm_t,
    load_sems,
    send_sems,
    recv_sems,
):
    rows, width = tokens.shape
    chips = ep // 2
    me = lax.axis_index("ep")
    z, core = me // 2, lax.rem(me, 2)

    def wrap(i):
        return lax.rem(i + 2 * chips, chips)

    def dev(zz, cc):
        return {"ep": wrap(zz) * 2 + cc}

    barrier = pltpu.get_barrier_semaphore()

    def hello(i, carry):
        pl.semaphore_signal(
            barrier, inc=1, device_id={"ep": lax.rem(me + i, ep)}, device_id_type=MESH
        )
        return carry

    lax.fori_loop(1, ep, hello, 0)

    half = w_q.shape[1]
    loads = [
        pltpu.make_async_copy(w_q, own_w.at[0, :, pl.ds(0, half)], load_sems.at[0]),
        pltpu.make_async_copy(w_k, own_w.at[0, :, pl.ds(half, half)], load_sems.at[1]),
        pltpu.make_async_copy(w_v, own_w.at[1], load_sems.at[2]),
        pltpu.make_async_copy(state, st, load_sems.at[3]),
        pltpu.make_async_copy(w_out, wo, load_sems.at[4]),
        pltpu.make_async_copy(w_gate.at[0], wg, load_sems.at[5]),
        pltpu.make_async_copy(w_lin.at[0], wl, load_sems.at[6]),
        pltpu.make_async_copy(w_down.at[0], wd, load_sems.at[7]),
    ]
    for c in loads:
        c.start()

    tok = tokens[...].astype(F32)
    normed = rms(tok, g_mix[...]).astype(BF16)
    for i in range(chips + 2):
        j = (i - 1) % chips
        xs[i] = normed[:, 128 * j : 128 * (j + 1)]

    for c in loads[:3]:
        c.wait()

    pl.semaphore_wait(barrier, ep - 1)

    def copy(src, dst, phase, device):
        return pltpu.make_async_remote_copy(
            src_ref=src,
            dst_ref=dst,
            send_sem=send_sems.at[phase],
            recv_sem=recv_sems.at[phase],
            device_id=device,
            device_id_type=MESH,
        )

    for oi in SEND_ORDER[:-1]:
        o = OFFSETS[oi]
        zz = wrap(z + o)
        for cc in range(2):
            slot = 3 * (2 * oi + core)
            if o == 8:
                copy(
                    xs.at[pl.ds(zz + 1, 1)],
                    xbuf.at[pl.ds(slot + 1, 1)],
                    0,
                    dev(zz, cc),
                ).start()
            else:
                copy(
                    xs.at[pl.ds(zz, 3)], xbuf.at[pl.ds(slot, 3)], 0, dev(zz, cc)
                ).start()
    copy(xs.at[pl.ds(z, 3)], xbuf.at[pl.ds(3 * core, 3)], 0, dev(z, 1 - core)).start()
    for n in (1, -1):
        for cc in range(2):
            copy(own_w.at[cc], wbuf.at[2 * (1 - n) + core], 1, dev(z + n, cc)).start()
    copy(own_w.at[1 - core], wbuf.at[2 + core], 1, dev(z, 1 - core)).start()

    xbuf[pl.ds(3 * core, 3)] = xs[pl.ds(z, 3)]
    wbuf[2 + core] = own_w[core]
    for cc in range(2):
        empty = jnp.zeros(xbuf.shape[1:], BF16)
        xbuf[3 * (10 + cc)] = empty
        xbuf[3 * (10 + cc) + 2] = empty

    low_rank = dot(normed, w_dd[...], (((1,), (1,)), ((), ()))).astype(BF16)
    pre = dot(low_rank, w_du[...]) + d_bias[...]
    log_decay = (jnp.minimum(pre, 0.0) - jnp.log1p(jnp.exp(-jnp.abs(pre)))) / TAU
    decay = jnp.exp(log_decay)
    decay_out[...] = decay

    kbs = 8
    tall = kbs * rows
    wide = ep * CAP * kbs
    r_t = lax.rem(iota((tall, rows), 0), rows)
    spread = (r_t == iota((tall, rows), 1)).astype(F32)
    route_rows = dot(
        spread, routes[...].astype(F32), (((1,), (1,)), ((), ())), lax.Precision.HIGHEST
    )
    sc = scores[...]
    e_sc = jnp.exp(sc - jnp.max(sc, axis=0, keepdims=True))
    weights = e_sc / jnp.sum(e_sc, axis=0, keepdims=True)
    weight_rows = dot(spread, weights, (((1,), (1,)), ((), ())), lax.Precision.HIGHEST)
    col = iota((tall, wide), 1)
    row = iota((tall, wide), 0)
    col_e = (col // (CAP * kbs)).astype(F32)
    col_slot = (lax.rem(col, CAP * kbs) // kbs).astype(F32)
    has = jnp.zeros((tall, wide), F32)
    weighted = jnp.zeros((tall, wide), F32)
    for j in range(routes.shape[0]):
        hit = (route_rows[:, j : j + 1] == col_e).astype(F32)
        has += hit
        weighted += hit * weight_rows[:, j : j + 1]
    rr, rc = iota((tall, tall), 0), iota((tall, tall), 1)
    before = (rr // rows == rc // rows) & (rc < rr)
    rank = dot(before.astype(BF16), has.astype(BF16))
    pick = has * (rank == col_slot).astype(F32) * (row // rows == lax.rem(col, kbs)).astype(F32)
    combine = weighted * pick
    combine_hi = combine.astype(BF16)
    combine_lo = (combine - combine_hi.astype(F32)).astype(BF16)
    pick = pick.astype(BF16)

    p_r, p_c = iota((wide, wide), 0), iota((wide, wide), 1)
    slots = ep * CAP
    q = lax.rem(p_r, slots)
    perm[...] = (p_c == (q * kbs + p_r // slots)).astype(F32).astype(BF16)
    q = lax.rem(p_c, slots)
    perm_t[...] = (p_r == (q * kbs + p_c // slots)).astype(F32).astype(BF16)

    others = 2 * len(OFFSETS) - 1
    units = 3 * (others - 2) + 2
    pltpu.make_async_copy(
        xs.at[pl.ds(0, units)] if units <= xs.shape[0] else xbuf.at[pl.ds(0, units)],
        xbuf.at[pl.ds(0, units)],
        recv_sems.at[0],
    ).wait()
    pltpu.make_async_copy(
        wbuf.at[pl.ds(0, 5)], wbuf.at[pl.ds(0, 5)], recv_sems.at[1]
    ).wait()
    chunks = 2 * len(OFFSETS)
    cols = wbuf.shape[2]
    part = None
    for n in range(3):
        x = jnp.concatenate(
            [xbuf[3 * i + n].astype(F32) for i in range(chunks)], axis=0
        ).astype(BF16)
        w = wbuf[2 * n : 2 * n + 2].reshape(2 * wbuf.shape[1], cols)
        p = dot(x, w)
        part = p if part is None else part + p
    for i in range(chunks):
        one = part[rows * i : rows * (i + 1)]
        psend[i] = jnp.concatenate(
            [one[:, : cols // 2], one[:, cols // 2 :]], axis=0
        ).astype(BF16)
    for oi in SEND_ORDER[:-1]:
        o = OFFSETS[oi]
        for cc in range(2):
            copy(psend.at[2 * oi + cc], rbuf.at[2 * oi + core], 2, dev(z - o, cc)).start()
    copy(psend.at[1 - core], rbuf.at[core], 2, dev(z, 1 - core)).start()
    rbuf[core] = psend[core]
    pltpu.make_async_copy(
        psend.at[pl.ds(0, others)], rbuf.at[pl.ds(0, others)], recv_sems.at[2]
    ).wait()

    sums = []
    for h in range(2):
        total = rbuf[h].astype(F32)
        for oi in range(1, len(OFFSETS)):
            total += rbuf[2 * oi + h].astype(F32)
        sums.append(total)
    queries = sums[0][:rows] * DK ** (-0.5)
    keys = sums[0][rows:]
    values = jnp.concatenate([sums[1][:rows], sums[1][rows:]], axis=1)
    key_out[...] = keys
    value_out[...] = values

    loads[3].wait()
    qd = queries * decay
    qk = queries * keys
    block = iota((rows, rows * DK), 1) // DK == iota((rows, rows * DK), 0)
    gain = g_head[...]
    headed = []
    for h in range(HEADS):
        q_h = qd[:, DK * h : DK * (h + 1)]
        lhs = jnp.where(block, jnp.concatenate([q_h] * rows, axis=1), 0.0)
        s_h = st[:, h].reshape(rows * DK, DV)
        a_h = dot(lhs, s_h, precision=lax.Precision.HIGHEST)
        a_h += jnp.sum(qk[:, DK * h : DK * (h + 1)], axis=1, keepdims=True) * values[
            :, DV * h : DV * (h + 1)
        ]
        headed.append(rms(a_h, gain).astype(BF16))
    headed = jnp.concatenate(headed, axis=1)

    loads[4].wait()
    residual = (tok + dot(headed, wo[...])).astype(BF16).astype(F32)
    fed = rms(residual, g_ffn[...])

    lanes = width // kbs
    fed_rows = jnp.concatenate(
        [fed[:, lanes * k : lanes * (k + 1)] for k in range(kbs)], axis=0
    ).astype(BF16)
    dsend[...] = (
        dot(pick, fed_rows, (((0,), (0,)), ((), ()))).astype(BF16).reshape(dsend.shape)
    )

    def exchange(src, dst, phase):
        def to(zz, cc):
            there = wrap(zz) * 2 + cc
            copy(src.at[there], dst.at[me], phase, {"ep": there}).start()

        for cc in range(2):
            to(z + chips // 2, cc)

        def step(i, carry):
            d = chips // 2 - i
            for cc in range(2):
                to(z + d, cc)
                to(z - d, cc)
            return carry

        lax.fori_loop(1, chips // 2, step, 0)
        to(z, 1 - core)
        dst[me] = src[me]
        pltpu.make_async_copy(
            src.at[pl.ds(0, ep - 1)], dst.at[pl.ds(0, ep - 1)], recv_sems.at[phase]
        ).wait()

    exchange(dsend, drecv, 3)

    arrived = dot(perm[...], drecv[...].reshape(wide, lanes)).astype(BF16)
    for k in range(kbs):
        xin[:, lanes * k : lanes * (k + 1)] = arrived[slots * k : slots * (k + 1)]
    loads[5].wait()
    loads[6].wait()
    tile = 256

    def up(i, carry):
        at = pl.ds(pl.multiple_of(i * tile, tile), tile)
        x = xin[...]
        gate = jnp.minimum(dot(x, wg[:, at]), LIMIT)
        lin = jnp.clip(dot(x, wl[:, at]), -LIMIT, LIMIT)
        hid[:, at] = (gate * jax.nn.sigmoid(ALPHA * gate) * (lin + 1.0)).astype(BF16)
        return carry

    lax.fori_loop(0, wg.shape[1] // tile, up, 0)
    loads[7].wait()
    for k in range(kbs):
        eo[slots * k : slots * (k + 1)] = dot(
            hid[...], wd[:, lanes * k : lanes * (k + 1)]
        ).astype(BF16)
    rsend[...] = dot(perm_t[...], eo[...]).astype(BF16).reshape(rsend.shape)

    exchange(rsend, rrecv, 4)

    back = rrecv[...].reshape(wide, lanes)
    mixed = dot(combine_hi, back) + dot(combine_lo, back)
    for k in range(kbs):
        at = slice(lanes * k, lanes * (k + 1))
        out[:, at] = (residual[:, at] + mixed[rows * k : rows * (k + 1)]).astype(BF16)

    pltpu.make_async_copy(
        xbuf.at[pl.ds(0, units)], xbuf.at[pl.ds(0, units)], send_sems.at[0]
    ).wait()
    pltpu.make_async_copy(wbuf.at[pl.ds(0, 5)], wbuf.at[pl.ds(0, 5)], send_sems.at[1]).wait()
    pltpu.make_async_copy(
        psend.at[pl.ds(0, others)], rbuf.at[pl.ds(0, others)], send_sems.at[2]
    ).wait()
    for src, dst, phase in ((dsend, drecv, 3), (rsend, rrecv, 4)):
        pltpu.make_async_copy(
            src.at[pl.ds(0, ep - 1)], dst.at[pl.ds(0, ep - 1)], send_sems.at[phase]
        ).wait()


def per_device(
    ep,
    tokens,
    state,
    g_mix,
    w_query,
    w_key,
    w_value,
    w_decay_down,
    w_decay_up,
    decay_bias,
    g_head,
    w_out,
    g_ffn,
    routes,
    route_scores,
    w_gate_in,
    w_lin_in,
    w_down,
):
    rows, width = tokens.shape
    share, qk = w_query.shape
    vw = w_value.shape[1]
    ff = w_gate_in.shape[2]
    lanes = width // 8
    wide = ep * CAP * 8
    vmem = pl.BlockSpec(memory_space=pltpu.VMEM)
    hbm = pl.BlockSpec(memory_space=pl.ANY)
    chunks = 2 * len(OFFSETS)
    output, keys, values, decay = pl.pallas_call(
        functools.partial(kernel, ep),
        out_shape=(
            jax.ShapeDtypeStruct((rows, width), BF16),
            jax.ShapeDtypeStruct((rows, qk), F32),
            jax.ShapeDtypeStruct((rows, vw), F32),
            jax.ShapeDtypeStruct((rows, qk), F32),
        ),
        in_specs=[vmem] * 9 + [hbm] * 8,
        out_specs=(vmem,) * 4,
        scratch_shapes=[
            pltpu.VMEM((2, share, vw), BF16),
            pltpu.VMEM(state.shape, F32),
            pltpu.VMEM(w_out.shape, BF16),
            pltpu.VMEM(w_gate_in.shape[1:], BF16),
            pltpu.VMEM(w_lin_in.shape[1:], BF16),
            pltpu.VMEM(w_down.shape[1:], BF16),
            pltpu.VMEM((ep // 2 + 2, rows, 2 * share), BF16),
            pltpu.VMEM((3 * chunks, rows, 2 * share), BF16),
            pltpu.VMEM((6, share, vw), BF16),
            pltpu.VMEM((chunks, 2 * rows, vw // 2), BF16),
            pltpu.VMEM((chunks, 2 * rows, vw // 2), BF16),
            pltpu.VMEM((ep, CAP * 8, lanes), BF16),
            pltpu.VMEM((ep, CAP * 8, lanes), BF16),
            pltpu.VMEM((ep, CAP * 8, lanes), BF16),
            pltpu.VMEM((ep, CAP * 8, lanes), BF16),
            pltpu.VMEM((ep * CAP, width), BF16),
            pltpu.VMEM((ep * CAP, ff), BF16),
            pltpu.VMEM((wide, lanes), BF16),
            pltpu.VMEM((wide, wide), BF16),
            pltpu.VMEM((wide, wide), BF16),
            pltpu.SemaphoreType.DMA((8,)),
            pltpu.SemaphoreType.DMA((5,)),
            pltpu.SemaphoreType.DMA((5,)),
        ],
        compiler_params=pltpu.CompilerParams(
            collective_id=0, has_side_effects=True, vmem_limit_bytes=48 * 1024 * 1024
        ),
        name="layer",
    )(
        tokens,
        g_mix.reshape(1, width),
        w_decay_down.T,
        w_decay_up,
        decay_bias.reshape(1, qk),
        g_head.reshape(1, DV),
        g_ffn.reshape(1, width),
        routes.T,
        route_scores.T,
        state,
        w_query,
        w_key,
        w_value,
        w_out,
        w_gate_in,
        w_lin_in,
        w_down,
    )
    decay = decay.reshape(rows, HEADS, DK)
    keys = keys.reshape(rows, HEADS, DK)
    values = values.reshape(rows, HEADS, DV)
    new_state = decay[..., None] * state + keys[..., None] * values[:, :, None, :]
    return (output, new_state)


def solution(mesh):
    shard = P(("grp", "ep"), None)
    experts = P("ep", None, None)
    return jax.shard_map(
        functools.partial(per_device, mesh.shape["ep"]),
        mesh=mesh,
        in_specs=(
            shard,
            P(("grp", "ep"), None, None, None),
            P(),
            P("ep", None),
            P("ep", None),
            P("ep", None),
            P(),
            P(),
            P(),
            P(),
            P(),
            P(),
            shard,
            shard,
            experts,
            experts,
            experts,
        ),
        out_specs=(shard, P(("grp", "ep"), None, None, None)),
        check_vma=False,
    )
```

```python
import functools

import jax
import jax.numpy as jnp
from jax import lax
from jax.experimental import pallas as pl
from jax.experimental.pallas import tpu as pltpu
from jax.sharding import PartitionSpec as P

MESH = pl.DeviceIdType.MESH
F32 = jnp.float32
BF16 = jnp.bfloat16

HEADS = 8
DK = 64
DV = 128
CAP = 2
EPS = 1e-06
TAU = 16.0
ALPHA = 1.702
LIMIT = 7.0

OFFSETS = (0, 3, -3, 6, -6, 8)
SEND_ORDER = (5, 3, 4, 1, 2, 0)


def rms(values, gain):
    return values * lax.rsqrt(jnp.mean(values * values, axis=-1, keepdims=True) + EPS) * gain


def dot(a, b, dims=None, precision=None):
    dims = dims or (((1,), (0,)), ((), ()))
    return lax.dot_general(a, b, dims, precision=precision, preferred_element_type=F32)


def iota(shape, dim):
    return lax.broadcasted_iota(jnp.int32, shape, dim)


def kernel(
    ep,
    tokens_in,
    g_mix_in,
    w_dd_in,
    w_du_in,
    d_bias_in,
    g_head_in,
    g_ffn_in,
    routes_in,
    scores_in,
    state,
    w_q,
    w_k,
    w_v,
    w_out,
    w_gate,
    w_lin,
    w_down,
    out,
    state_out,
    tokens,
    g_mix,
    w_dd,
    w_du,
    d_bias,
    g_head,
    g_ffn,
    routes,
    scores,
    own_w,
    st,
    wo,
    wg,
    wl,
    wd,
    xs,
    xbuf,
    wbuf,
    psend,
    rbuf,
    dsend,
    drecv,
    rsend,
    rrecv,
    xin,
    hid,
    eo,
    perm,
    perm_t,
    load_sems,
    send_sems,
    recv_sems,
):
    rows, width = tokens.shape
    chips = ep // 2
    me = lax.axis_index("ep")
    z, core = me // 2, lax.rem(me, 2)

    def wrap(i):
        return lax.rem(i + 2 * chips, chips)

    def dev(zz, cc):
        return {"ep": wrap(zz) * 2 + cc}

    half = w_q.shape[1]
    pairs = [
        (tokens_in, tokens),
        (g_mix_in, g_mix),
        (w_q, own_w.at[0, :, pl.ds(0, half)]),
        (w_k, own_w.at[0, :, pl.ds(half, half)]),
        (w_v, own_w.at[1]),
        (w_dd_in, w_dd),
        (w_du_in, w_du),
        (d_bias_in, d_bias),
        (routes_in, routes),
        (scores_in, scores),
        (g_head_in, g_head),
        (g_ffn_in, g_ffn),
        (state, st),
        (w_out, wo),
        (w_gate.at[0], wg),
        (w_lin.at[0], wl),
        (w_down.at[0], wd),
    ]
    loads = [
        pltpu.make_async_copy(src, dst, load_sems.at[i]) for i, (src, dst) in enumerate(pairs)
    ]
    for c in loads[:5]:
        c.start()

    barrier = pltpu.get_barrier_semaphore()

    def hello(i, carry):
        pl.semaphore_signal(
            barrier, inc=1, device_id={"ep": lax.rem(me + i, ep)}, device_id_type=MESH
        )
        return carry

    with jax.named_scope("hello"):
        lax.fori_loop(1, ep, hello, 0)
        for c in loads[5:]:
            c.start()
        for c in loads[:2]:
            c.wait()

    tok = tokens[...].astype(F32)
    normed = rms(tok, g_mix[...]).astype(BF16)
    for i in range(chips + 2):
        j = (i - 1) % chips
        xs[i] = normed[:, 128 * j : 128 * (j + 1)]

    for c in loads[2:5]:
        c.wait()

    with jax.named_scope("barrier"):
        pl.semaphore_wait(barrier, ep - 1)

    def copy(src, dst, phase, device):
        return pltpu.make_async_remote_copy(
            src_ref=src,
            dst_ref=dst,
            send_sem=send_sems.at[phase],
            recv_sem=recv_sems.at[phase],
            device_id=device,
            device_id_type=MESH,
        )

    for oi in SEND_ORDER[:-1]:
        o = OFFSETS[oi]
        zz = wrap(z + o)
        for cc in range(2):
            slot = 3 * (2 * oi + core)
            if o == 8:
                copy(
                    xs.at[pl.ds(zz + 1, 1)],
                    xbuf.at[pl.ds(slot + 1, 1)],
                    0,
                    dev(zz, cc),
                ).start()
            else:
                copy(
                    xs.at[pl.ds(zz, 3)], xbuf.at[pl.ds(slot, 3)], 0, dev(zz, cc)
                ).start()
    copy(xs.at[pl.ds(z, 3)], xbuf.at[pl.ds(3 * core, 3)], 0, dev(z, 1 - core)).start()
    for n in (1, -1):
        for cc in range(2):
            copy(own_w.at[cc], wbuf.at[2 * (1 - n) + core], 1, dev(z + n, cc)).start()
    copy(own_w.at[1 - core], wbuf.at[2 + core], 1, dev(z, 1 - core)).start()

    xbuf[pl.ds(3 * core, 3)] = xs[pl.ds(z, 3)]
    wbuf[2 + core] = own_w[core]
    for cc in range(2):
        empty = jnp.zeros(xbuf.shape[1:], BF16)
        xbuf[3 * (10 + cc)] = empty
        xbuf[3 * (10 + cc) + 2] = empty

    for c in loads[5:12]:
        c.wait()
    low_rank = dot(normed, w_dd[...], (((1,), (1,)), ((), ()))).astype(BF16)
    pre = dot(low_rank, w_du[...]) + d_bias[...]
    log_decay = (jnp.minimum(pre, 0.0) - jnp.log1p(jnp.exp(-jnp.abs(pre)))) / TAU
    decay = jnp.exp(log_decay)

    kbs = 8
    tall = kbs * rows
    wide = ep * CAP * kbs
    r_t = lax.rem(iota((tall, rows), 0), rows)
    spread = (r_t == iota((tall, rows), 1)).astype(F32)
    route_rows = dot(
        spread, routes[...].astype(F32), (((1,), (1,)), ((), ())), lax.Precision.HIGHEST
    )
    sc = scores[...]
    e_sc = jnp.exp(sc - jnp.max(sc, axis=0, keepdims=True))
    weights = e_sc / jnp.sum(e_sc, axis=0, keepdims=True)
    weight_rows = dot(spread, weights, (((1,), (1,)), ((), ())), lax.Precision.HIGHEST)
    col = iota((tall, wide), 1)
    row = iota((tall, wide), 0)
    col_e = (col // (CAP * kbs)).astype(F32)
    col_slot = (lax.rem(col, CAP * kbs) // kbs).astype(F32)
    has = jnp.zeros((tall, wide), F32)
    weighted = jnp.zeros((tall, wide), F32)
    for j in range(routes.shape[0]):
        hit = (route_rows[:, j : j + 1] == col_e).astype(F32)
        has += hit
        weighted += hit * weight_rows[:, j : j + 1]
    rr, rc = iota((tall, tall), 0), iota((tall, tall), 1)
    before = (rr // rows == rc // rows) & (rc < rr)
    rank = dot(before.astype(BF16), has.astype(BF16))
    pick = has * (rank == col_slot).astype(F32) * (row // rows == lax.rem(col, kbs)).astype(F32)
    combine = weighted * pick
    combine_hi = combine.astype(BF16)
    combine_lo = (combine - combine_hi.astype(F32)).astype(BF16)
    pick = pick.astype(BF16)

    p_r, p_c = iota((wide, wide), 0), iota((wide, wide), 1)
    slots = ep * CAP
    q = lax.rem(p_r, slots)
    perm[...] = (p_c == (q * kbs + p_r // slots)).astype(F32).astype(BF16)
    q = lax.rem(p_c, slots)
    perm_t[...] = (p_r == (q * kbs + p_c // slots)).astype(F32).astype(BF16)

    others = 2 * len(OFFSETS) - 1
    units = 3 * (others - 2) + 2
    with jax.named_scope("tokens_wait"):
        pltpu.make_async_copy(
            xbuf.at[pl.ds(0, units)], xbuf.at[pl.ds(0, units)], recv_sems.at[0]
        ).wait()
    with jax.named_scope("weights_wait"):
        pltpu.make_async_copy(
            wbuf.at[pl.ds(0, 5)], wbuf.at[pl.ds(0, 5)], recv_sems.at[1]
        ).wait()
    chunks = 2 * len(OFFSETS)
    cols = wbuf.shape[2]
    part = None
    for n in range(3):
        x = jnp.concatenate(
            [xbuf[3 * i + n].astype(F32) for i in range(chunks)], axis=0
        ).astype(BF16)
        w = wbuf[2 * n : 2 * n + 2].reshape(2 * wbuf.shape[1], cols)
        p = dot(x, w)
        part = p if part is None else part + p
    for i in range(chunks):
        one = part[rows * i : rows * (i + 1)]
        psend[i] = jnp.concatenate(
            [one[:, : cols // 2], one[:, cols // 2 :]], axis=0
        ).astype(BF16)
    for oi in SEND_ORDER[:-1]:
        o = OFFSETS[oi]
        for cc in range(2):
            copy(psend.at[2 * oi + cc], rbuf.at[2 * oi + core], 2, dev(z - o, cc)).start()
    copy(psend.at[1 - core], rbuf.at[core], 2, dev(z, 1 - core)).start()
    rbuf[core] = psend[core]
    with jax.named_scope("partials_wait"):
        pltpu.make_async_copy(
            psend.at[pl.ds(0, others)], rbuf.at[pl.ds(0, others)], recv_sems.at[2]
        ).wait()

    sums = []
    for h in range(2):
        total = rbuf[h].astype(F32)
        for oi in range(1, len(OFFSETS)):
            total += rbuf[2 * oi + h].astype(F32)
        sums.append(total)
    queries = sums[0][:rows] * DK ** (-0.5)
    keys = sums[0][rows:]
    values = jnp.concatenate([sums[1][:rows], sums[1][rows:]], axis=1)

    loads[12].wait()
    qd = queries * decay
    qk = queries * keys
    block = iota((rows, rows * DK), 1) // DK == iota((rows, rows * DK), 0)
    gain = g_head[...]
    headed = []
    for h in range(HEADS):
        q_h = qd[:, DK * h : DK * (h + 1)]
        lhs = jnp.where(block, jnp.concatenate([q_h] * rows, axis=1), 0.0)
        s_h = st[:, h].reshape(rows * DK, DV)
        a_h = dot(lhs, s_h, precision=lax.Precision.HIGHEST)
        a_h += jnp.sum(qk[:, DK * h : DK * (h + 1)], axis=1, keepdims=True) * values[
            :, DV * h : DV * (h + 1)
        ]
        headed.append(rms(a_h, gain).astype(BF16))
    headed = jnp.concatenate(headed, axis=1)

    loads[13].wait()
    residual = (tok + dot(headed, wo[...])).astype(BF16).astype(F32)
    fed = rms(residual, g_ffn[...])

    lanes = width // kbs
    fed_rows = jnp.concatenate(
        [fed[:, lanes * k : lanes * (k + 1)] for k in range(kbs)], axis=0
    ).astype(BF16)
    dsend[...] = (
        dot(pick, fed_rows, (((0,), (0,)), ((), ()))).astype(BF16).reshape(dsend.shape)
    )

    def exchange(src, dst, phase):
        def to(zz, cc):
            there = wrap(zz) * 2 + cc
            copy(src.at[there], dst.at[me], phase, {"ep": there}).start()

        for cc in range(2):
            to(z + chips // 2, cc)

        def step(i, carry):
            d = chips // 2 - i
            for cc in range(2):
                to(z + d, cc)
                to(z - d, cc)
            return carry

        lax.fori_loop(1, chips // 2, step, 0)
        to(z, 1 - core)
        dst[me] = src[me]

    def arrive(src, dst, phase):
        pltpu.make_async_copy(
            src.at[pl.ds(0, ep - 1)], dst.at[pl.ds(0, ep - 1)], recv_sems.at[phase]
        ).wait()

    with jax.named_scope("dispatch"):
        exchange(dsend, drecv, 3)

    with jax.named_scope("new_state"):
        decay_cols, key_cols = decay.T, keys.T
        for t in range(rows):
            for h in range(HEADS):
                at = slice(DK * h, DK * (h + 1))
                st[t, h] = (
                    decay_cols[at, t : t + 1] * st[t, h]
                    + key_cols[at, t : t + 1] * values[t : t + 1, DV * h : DV * (h + 1)]
                )

        store = pltpu.make_async_copy(st, state_out, load_sems.at[12])
        store.start()

    with jax.named_scope("dispatch_wait"):
        arrive(dsend, drecv, 3)

    arrived = dot(perm[...], drecv[...].reshape(wide, lanes)).astype(BF16)
    for k in range(kbs):
        xin[:, lanes * k : lanes * (k + 1)] = arrived[slots * k : slots * (k + 1)]
    loads[14].wait()
    loads[15].wait()
    tile = 256

    def up(i, carry):
        at = pl.ds(pl.multiple_of(i * tile, tile), tile)
        x = xin[...]
        gate = jnp.minimum(dot(x, wg[:, at]), LIMIT)
        lin = jnp.clip(dot(x, wl[:, at]), -LIMIT, LIMIT)
        hid[:, at] = (gate * jax.nn.sigmoid(ALPHA * gate) * (lin + 1.0)).astype(BF16)
        return carry

    lax.fori_loop(0, wg.shape[1] // tile, up, 0)
    loads[16].wait()
    for k in range(kbs):
        eo[slots * k : slots * (k + 1)] = dot(
            hid[...], wd[:, lanes * k : lanes * (k + 1)]
        ).astype(BF16)
    rsend[...] = dot(perm_t[...], eo[...]).astype(BF16).reshape(rsend.shape)

    with jax.named_scope("back"):
        exchange(rsend, rrecv, 4)
    with jax.named_scope("back_wait"):
        arrive(rsend, rrecv, 4)

    back = rrecv[...].reshape(wide, lanes)
    mixed = dot(combine_hi, back) + dot(combine_lo, back)
    for k in range(kbs):
        at = slice(lanes * k, lanes * (k + 1))
        out[:, at] = (residual[:, at] + mixed[rows * k : rows * (k + 1)]).astype(BF16)

    store.wait()
    pltpu.make_async_copy(
        xbuf.at[pl.ds(0, units)], xbuf.at[pl.ds(0, units)], send_sems.at[0]
    ).wait()
    pltpu.make_async_copy(wbuf.at[pl.ds(0, 5)], wbuf.at[pl.ds(0, 5)], send_sems.at[1]).wait()
    pltpu.make_async_copy(
        psend.at[pl.ds(0, others)], rbuf.at[pl.ds(0, others)], send_sems.at[2]
    ).wait()
    for src, dst, phase in ((dsend, drecv, 3), (rsend, rrecv, 4)):
        pltpu.make_async_copy(
            src.at[pl.ds(0, ep - 1)], dst.at[pl.ds(0, ep - 1)], send_sems.at[phase]
        ).wait()


def per_device(
    ep,
    tokens,
    state,
    g_mix,
    w_query,
    w_key,
    w_value,
    w_decay_down,
    w_decay_up,
    decay_bias,
    g_head,
    w_out,
    g_ffn,
    routes,
    route_scores,
    w_gate_in,
    w_lin_in,
    w_down,
):
    rows, width = tokens.shape
    share, qk = w_query.shape
    vw = w_value.shape[1]
    ff = w_gate_in.shape[2]
    lanes = width // 8
    wide = ep * CAP * 8
    vmem = pl.BlockSpec(memory_space=pltpu.VMEM)
    hbm = pl.BlockSpec(memory_space=pltpu.HBM)
    chunks = 2 * len(OFFSETS)
    return pl.pallas_call(
        functools.partial(kernel, ep),
        out_shape=(
            jax.ShapeDtypeStruct((rows, width), BF16),
            jax.ShapeDtypeStruct(state.shape, F32),
        ),
        in_specs=[hbm] * 17,
        out_specs=(vmem, hbm),
        scratch_shapes=[
            pltpu.VMEM((rows, width), BF16),
            pltpu.VMEM((1, width), F32),
            pltpu.VMEM(w_decay_down.shape[::-1], BF16),
            pltpu.VMEM(w_decay_up.shape, BF16),
            pltpu.VMEM((1, qk), F32),
            pltpu.VMEM((1, DV), F32),
            pltpu.VMEM((1, width), F32),
            pltpu.VMEM(routes.shape[::-1], jnp.int32),
            pltpu.VMEM(route_scores.shape[::-1], F32),
            pltpu.VMEM((2, share, vw), BF16),
            pltpu.VMEM(state.shape, F32),
            pltpu.VMEM(w_out.shape, BF16),
            pltpu.VMEM(w_gate_in.shape[1:], BF16),
            pltpu.VMEM(w_lin_in.shape[1:], BF16),
            pltpu.VMEM(w_down.shape[1:], BF16),
            pltpu.VMEM((ep // 2 + 2, rows, 2 * share), BF16),
            pltpu.VMEM((3 * chunks, rows, 2 * share), BF16),
            pltpu.VMEM((6, share, vw), BF16),
            pltpu.VMEM((chunks, 2 * rows, vw // 2), BF16),
            pltpu.VMEM((chunks, 2 * rows, vw // 2), BF16),
            pltpu.VMEM((ep, CAP * 8, lanes), BF16),
            pltpu.VMEM((ep, CAP * 8, lanes), BF16),
            pltpu.VMEM((ep, CAP * 8, lanes), BF16),
            pltpu.VMEM((ep, CAP * 8, lanes), BF16),
            pltpu.VMEM((ep * CAP, width), BF16),
            pltpu.VMEM((ep * CAP, ff), BF16),
            pltpu.VMEM((wide, lanes), BF16),
            pltpu.VMEM((wide, wide), BF16),
            pltpu.VMEM((wide, wide), BF16),
            pltpu.SemaphoreType.DMA((17,)),
            pltpu.SemaphoreType.DMA((5,)),
            pltpu.SemaphoreType.DMA((5,)),
        ],
        compiler_params=pltpu.CompilerParams(
            collective_id=0, has_side_effects=True, vmem_limit_bytes=63_000_000
        ),
        name="layer",
    )(
        tokens,
        g_mix.reshape(1, width),
        w_decay_down.T,
        w_decay_up,
        decay_bias.reshape(1, qk),
        g_head.reshape(1, DV),
        g_ffn.reshape(1, width),
        routes.T,
        route_scores.T,
        state,
        w_query,
        w_key,
        w_value,
        w_out,
        w_gate_in,
        w_lin_in,
        w_down,
    )


def solution(mesh):
    shard = P(("grp", "ep"), None)
    experts = P("ep", None, None)
    return jax.shard_map(
        functools.partial(per_device, mesh.shape["ep"]),
        mesh=mesh,
        in_specs=(
            shard,
            P(("grp", "ep"), None, None, None),
            P(),
            P("ep", None),
            P("ep", None),
            P("ep", None),
            P(),
            P(),
            P(),
            P(),
            P(),
            P(),
            shard,
            shard,
            experts,
            experts,
            experts,
        ),
        out_specs=(shard, P(("grp", "ep"), None, None, None)),
        check_vma=False,
    )
```

```python
import functools

import jax
import jax.numpy as jnp
from jax import lax
from jax.experimental import pallas as pl
from jax.experimental.pallas import tpu as pltpu
from jax.sharding import PartitionSpec as P

MESH = pl.DeviceIdType.MESH
F32 = jnp.float32
BF16 = jnp.bfloat16

HEADS = 8
DK = 64
DV = 128
CAP = 2
EPS = 1e-06
TAU = 16.0
ALPHA = 1.702
LIMIT = 7.0

OFFSETS = (1, 4, 7, -2, -5, -7)
SEND_ORDER = (2, 5, 4, 1, 3, 0)
RING = (8, 7, -7, 6, -6, 5, -5, 4, -4, 3, -3, 2, -2, 1, -1, 0)


def rms(values, gain):
    return values * lax.rsqrt(jnp.mean(values * values, axis=-1, keepdims=True) + EPS) * gain


def dot(a, b, dims=None, precision=None):
    dims = dims or (((1,), (0,)), ((), ()))
    return lax.dot_general(a, b, dims, precision=precision, preferred_element_type=F32)


def iota(shape, dim):
    return lax.broadcasted_iota(jnp.int32, shape, dim)


def kernel(
    ep,
    tokens_in,
    g_mix_in,
    w_dd_in,
    w_du_in,
    d_bias_in,
    g_head_in,
    g_ffn_in,
    routes_in,
    scores_in,
    state,
    w_q,
    w_k,
    w_v,
    w_out,
    w_gate,
    w_lin,
    w_down,
    out,
    state_out,
    tokens,
    g_mix,
    w_dd,
    w_du,
    d_bias,
    g_head,
    g_ffn,
    routes,
    scores,
    own_w,
    st,
    wo,
    wg,
    wl,
    wd,
    xs,
    xbuf,
    wbuf,
    psend,
    rbuf,
    dsend,
    drecv,
    rsend,
    rrecv,
    xin,
    hid,
    eo,
    perm,
    perm_t,
    load_sems,
    send_sems,
    recv_sems,
):
    rows, width = tokens.shape
    chips = ep // 2
    me = lax.axis_index("ep")
    z, core = me // 2, lax.rem(me, 2)

    def wrap(i):
        return lax.rem(i + 2 * chips, chips)

    def dev(zz, cc):
        return {"ep": wrap(zz) * 2 + cc}

    half = w_q.shape[1]
    pairs = [
        (tokens_in, tokens),
        (g_mix_in, g_mix),
        (w_q, own_w.at[0, :, pl.ds(0, half)]),
        (w_k, own_w.at[0, :, pl.ds(half, half)]),
        (w_v, own_w.at[1]),
        (w_dd_in, w_dd),
        (w_du_in, w_du),
        (d_bias_in, d_bias),
        (routes_in, routes),
        (scores_in, scores),
        (g_head_in, g_head),
        (g_ffn_in, g_ffn),
        (state, st),
        (w_out, wo),
        (w_gate.at[0], wg),
        (w_lin.at[0], wl),
        (w_down.at[0], wd),
    ]
    loads = [
        pltpu.make_async_copy(src, dst, load_sems.at[i]) for i, (src, dst) in enumerate(pairs)
    ]
    for c in loads[:5]:
        c.start()

    barrier = pltpu.get_barrier_semaphore()

    def hello(i, carry):
        pl.semaphore_signal(
            barrier, inc=1, device_id={"ep": lax.rem(me + i, ep)}, device_id_type=MESH
        )
        return carry

    with jax.named_scope("hello"):
        lax.fori_loop(1, ep, hello, 0)
        for c in loads[5:]:
            c.start()
        for c in loads[:2]:
            c.wait()

    tok = tokens[...].astype(F32)
    normed = rms(tok, g_mix[...]).astype(BF16)
    for i in range(chips + 2):
        j = (i - 1) % chips
        xs[i] = normed[:, 128 * j : 128 * (j + 1)]

    for c in loads[2:5]:
        c.wait()

    with jax.named_scope("barrier"):
        pl.semaphore_wait(barrier, ep - 1)

    def copy(src, dst, phase, device):
        return pltpu.make_async_remote_copy(
            src_ref=src,
            dst_ref=dst,
            send_sem=send_sems.at[phase],
            recv_sem=recv_sems.at[phase],
            device_id=device,
            device_id_type=MESH,
        )

    for oi in SEND_ORDER:
        for cc in range(2):
            zz = wrap(z + (1 - 2 * cc) * OFFSETS[oi])
            slot = 3 * (2 * oi + core)
            if oi == len(OFFSETS) - 1:
                src, dst = xs.at[pl.ds(zz + 1, 1)], xbuf.at[pl.ds(slot + 1, 1)]
            else:
                src, dst = xs.at[pl.ds(zz, 3)], xbuf.at[pl.ds(slot, 3)]
            copy(src, dst, 0, dev(zz, cc)).start()
    for n in (1, -1):
        for cc in range(2):
            copy(own_w.at[cc], wbuf.at[2 * (1 - n) + core], 1, dev(z + n, cc)).start()
    copy(own_w.at[1 - core], wbuf.at[2 + core], 1, dev(z, 1 - core)).start()

    wbuf[2 + core] = own_w[core]
    for cc in range(2):
        empty = jnp.zeros(xbuf.shape[1:], BF16)
        xbuf[3 * (10 + cc)] = empty
        xbuf[3 * (10 + cc) + 2] = empty

    for c in loads[5:12]:
        c.wait()
    low_rank = dot(normed, w_dd[...], (((1,), (1,)), ((), ()))).astype(BF16)
    pre = dot(low_rank, w_du[...]) + d_bias[...]
    log_decay = (jnp.minimum(pre, 0.0) - jnp.log1p(jnp.exp(-jnp.abs(pre)))) / TAU
    decay = jnp.exp(log_decay)

    kbs = 8
    tall = kbs * rows
    wide = ep * CAP * kbs
    r_t = lax.rem(iota((tall, rows), 0), rows)
    spread = (r_t == iota((tall, rows), 1)).astype(F32)
    route_rows = dot(
        spread, routes[...].astype(F32), (((1,), (1,)), ((), ())), lax.Precision.HIGHEST
    )
    sc = scores[...]
    e_sc = jnp.exp(sc - jnp.max(sc, axis=0, keepdims=True))
    weights = e_sc / jnp.sum(e_sc, axis=0, keepdims=True)
    weight_rows = dot(spread, weights, (((1,), (1,)), ((), ())), lax.Precision.HIGHEST)
    col = iota((tall, wide), 1)
    row = iota((tall, wide), 0)
    col_e = (col // (CAP * kbs)).astype(F32)
    col_slot = (lax.rem(col, CAP * kbs) // kbs).astype(F32)
    has = jnp.zeros((tall, wide), F32)
    weighted = jnp.zeros((tall, wide), F32)
    for j in range(routes.shape[0]):
        hit = (route_rows[:, j : j + 1] == col_e).astype(F32)
        has += hit
        weighted += hit * weight_rows[:, j : j + 1]
    rr, rc = iota((tall, tall), 0), iota((tall, tall), 1)
    before = (rr // rows == rc // rows) & (rc < rr)
    rank = dot(before.astype(BF16), has.astype(BF16))
    pick = has * (rank == col_slot).astype(F32) * (row // rows == lax.rem(col, kbs)).astype(F32)
    combine = weighted * pick
    combine_hi = combine.astype(BF16)
    combine_lo = (combine - combine_hi.astype(F32)).astype(BF16)
    pick = pick.astype(BF16)

    part_rows = wide // 2
    slots = part_rows // kbs
    p_r, p_c = iota((part_rows, part_rows), 0), iota((part_rows, part_rows), 1)
    perm[...] = (p_c == (lax.rem(p_r, slots) * kbs + p_r // slots)).astype(F32).astype(BF16)
    perm_t[...] = (p_r == (lax.rem(p_c, slots) * kbs + p_c // slots)).astype(F32).astype(BF16)

    chunks = 2 * len(OFFSETS)
    units = 3 * (chunks - 2) + 2
    with jax.named_scope("tokens_wait"):
        pltpu.make_async_copy(
            xbuf.at[pl.ds(0, units)], xbuf.at[pl.ds(0, units)], recv_sems.at[0]
        ).wait()
    with jax.named_scope("weights_wait"):
        pltpu.make_async_copy(
            wbuf.at[pl.ds(0, 5)], wbuf.at[pl.ds(0, 5)], recv_sems.at[1]
        ).wait()
    cols = wbuf.shape[2]
    part = None
    for n in range(3):
        x = jnp.concatenate(
            [xbuf[3 * i + n].astype(F32) for i in range(chunks)], axis=0
        ).astype(BF16)
        w = wbuf[2 * n : 2 * n + 2].reshape(2 * wbuf.shape[1], cols)
        p = dot(x, w)
        part = p if part is None else part + p
    for i in range(chunks):
        one = part[rows * i : rows * (i + 1)]
        psend[i] = jnp.concatenate(
            [one[:, : cols // 2], one[:, cols // 2 :]], axis=0
        ).astype(BF16)
    sign = 1 - 2 * core
    for oi in SEND_ORDER:
        for cc in range(2):
            to = dev(z - sign * OFFSETS[oi], cc)
            copy(psend.at[2 * oi + cc], rbuf.at[2 * oi + core], 2, to).start()
    with jax.named_scope("partials_wait"):
        pltpu.make_async_copy(
            psend, rbuf, recv_sems.at[2]
        ).wait()

    sums = []
    for h in range(2):
        total = rbuf[h].astype(F32)
        for oi in range(1, len(OFFSETS)):
            total += rbuf[2 * oi + h].astype(F32)
        sums.append(total)
    queries = sums[0][:rows] * DK ** (-0.5)
    keys = sums[0][rows:]
    values = jnp.concatenate([sums[1][:rows], sums[1][rows:]], axis=1)

    loads[12].wait()
    qd = queries * decay
    qk = queries * keys
    block = iota((rows, rows * DK), 1) // DK == iota((rows, rows * DK), 0)
    gain = g_head[...]
    headed = []
    for h in range(HEADS):
        q_h = qd[:, DK * h : DK * (h + 1)]
        lhs = jnp.where(block, jnp.concatenate([q_h] * rows, axis=1), 0.0)
        s_h = st[:, h].reshape(rows * DK, DV)
        a_h = dot(lhs, s_h, precision=lax.Precision.HIGHEST)
        a_h += jnp.sum(qk[:, DK * h : DK * (h + 1)], axis=1, keepdims=True) * values[
            :, DV * h : DV * (h + 1)
        ]
        headed.append(rms(a_h, gain).astype(BF16))
    headed = jnp.concatenate(headed, axis=1)

    loads[13].wait()
    residual = (tok + dot(headed, wo[...])).astype(BF16).astype(F32)
    fed = rms(residual, g_ffn[...])

    lanes = width // kbs
    fed_rows = jnp.concatenate(
        [fed[:, lanes * k : lanes * (k + 1)] for k in range(kbs)], axis=0
    ).astype(BF16)
    dsend[...] = (
        dot(pick, fed_rows, (((0,), (0,)), ((), ()))).astype(BF16).reshape(dsend.shape)
    )

    with jax.named_scope("dispatch"):
        for j, o in enumerate(RING):
            for cc in range(2):
                there = wrap(z + o) * 2 + cc
                if o:
                    copy(
                        dsend.at[there], drecv.at[2 * j + core], 3 + j // (ep // 4), {"ep": there}
                    ).start()
        there = 2 * z + 1 - core
        copy(dsend.at[there], drecv.at[ep - 2 + core], 4, {"ep": there}).start()
        drecv[ep - 2 + core] = dsend[me]

    with jax.named_scope("new_state"):
        decay_cols, key_cols = decay.T, keys.T
        for t in range(rows):
            for h in range(HEADS):
                at = slice(DK * h, DK * (h + 1))
                st[t, h] = (
                    decay_cols[at, t : t + 1] * st[t, h]
                    + key_cols[at, t : t + 1] * values[t : t + 1, DV * h : DV * (h + 1)]
                )

        store = pltpu.make_async_copy(st, state_out, load_sems.at[12])
        store.start()

    tile = 256
    near = ep // 2

    def expert(at):
        arrived = dot(perm[...], drecv[at : at + near].reshape(part_rows, lanes)).astype(BF16)
        for k in range(kbs):
            xin[:, lanes * k : lanes * (k + 1)] = arrived[slots * k : slots * (k + 1)]

        def up(i, carry):
            cols = pl.ds(pl.multiple_of(i * tile, tile), tile)
            x = xin[...]
            gate = jnp.minimum(dot(x, wg[:, cols]), LIMIT)
            lin = jnp.clip(dot(x, wl[:, cols]), -LIMIT, LIMIT)
            hid[:, cols] = (gate * jax.nn.sigmoid(ALPHA * gate) * (lin + 1.0)).astype(BF16)
            return carry

        lax.fori_loop(0, wg.shape[1] // tile, up, 0)
        for k in range(kbs):
            eo[slots * k : slots * (k + 1)] = dot(
                hid[...], wd[:, lanes * k : lanes * (k + 1)]
            ).astype(BF16)
        rsend[at : at + near] = (
            dot(perm_t[...], eo[...]).astype(BF16).reshape(near, CAP * kbs, lanes)
        )

    def send_back(j, o):
        for cc in range(2):
            copy(rsend.at[2 * j + cc], rrecv.at[me], 5, dev(z - o, cc)).start()

    with jax.named_scope("far_wait"):
        pltpu.make_async_copy(
            dsend.at[pl.ds(0, near)], drecv.at[pl.ds(0, near)], recv_sems.at[3]
        ).wait()
    for c in loads[14:]:
        c.wait()
    with jax.named_scope("far_expert"):
        expert(0)
    with jax.named_scope("far_back"):
        for j in range(near // 2):
            send_back(j, RING[j])
    with jax.named_scope("near_wait"):
        pltpu.make_async_copy(
            dsend.at[pl.ds(1, near - 1)], drecv.at[pl.ds(1, near - 1)], recv_sems.at[4]
        ).wait()
    with jax.named_scope("near_expert"):
        expert(near)
    with jax.named_scope("near_back"):
        for j in range(near // 2, near - 1):
            send_back(j, RING[j])
        copy(
            rsend.at[ep - 1 - core], rrecv.at[me], 5, dev(z, 1 - core)
        ).start()
        rrecv[me] = rsend[ep - 2 + core]
    with jax.named_scope("back_wait"):
        pltpu.make_async_copy(
            rsend.at[pl.ds(0, ep - 1)], rrecv.at[pl.ds(0, ep - 1)], recv_sems.at[5]
        ).wait()

    back = rrecv[...].reshape(wide, lanes)
    mixed = dot(combine_hi, back) + dot(combine_lo, back)
    for k in range(kbs):
        at = slice(lanes * k, lanes * (k + 1))
        out[:, at] = (residual[:, at] + mixed[rows * k : rows * (k + 1)]).astype(BF16)

    store.wait()
    pltpu.make_async_copy(
        xbuf.at[pl.ds(0, units)], xbuf.at[pl.ds(0, units)], send_sems.at[0]
    ).wait()
    pltpu.make_async_copy(wbuf.at[pl.ds(0, 5)], wbuf.at[pl.ds(0, 5)], send_sems.at[1]).wait()
    pltpu.make_async_copy(psend, rbuf, send_sems.at[2]).wait()
    pltpu.make_async_copy(
        dsend.at[pl.ds(0, ep // 2)], drecv.at[pl.ds(0, ep // 2)], send_sems.at[3]
    ).wait()
    pltpu.make_async_copy(
        dsend.at[pl.ds(1, ep // 2 - 1)], drecv.at[pl.ds(1, ep // 2 - 1)], send_sems.at[4]
    ).wait()
    pltpu.make_async_copy(
        rsend.at[pl.ds(0, ep - 1)], rrecv.at[pl.ds(0, ep - 1)], send_sems.at[5]
    ).wait()


def finish(out_in, state_in, out, state_out, out_buf, state_buf, in_sems, out_sems):
    rows = state_in.shape[0]
    ways = [(state_in.at[i], state_buf.at[i], state_out.at[i]) for i in range(rows)]
    ways.append((out_in, out_buf, out))
    ins = [pltpu.make_async_copy(w[0], w[1], in_sems.at[i]) for i, w in enumerate(ways)]
    outs = [pltpu.make_async_copy(w[1], w[2], out_sems.at[i]) for i, w in enumerate(ways)]
    for c in ins:
        c.start()
    for c, d in zip(ins, outs):
        c.wait()
        d.start()
    for d in outs:
        d.wait()


def per_device(
    ep,
    tokens,
    state,
    g_mix,
    w_query,
    w_key,
    w_value,
    w_decay_down,
    w_decay_up,
    decay_bias,
    g_head,
    w_out,
    g_ffn,
    routes,
    route_scores,
    w_gate_in,
    w_lin_in,
    w_down,
):
    rows, width = tokens.shape
    share, qk = w_query.shape
    vw = w_value.shape[1]
    ff = w_gate_in.shape[2]
    lanes = width // 8
    wide = ep * CAP * 8
    vmem = pl.BlockSpec(memory_space=pltpu.VMEM)
    hbm = pl.BlockSpec(memory_space=pltpu.HBM)
    chunks = 2 * len(OFFSETS)
    output, new_state = pl.pallas_call(
        functools.partial(kernel, ep),
        out_shape=(
            jax.ShapeDtypeStruct((rows, width), BF16),
            jax.ShapeDtypeStruct(state.shape, F32),
        ),
        in_specs=[hbm] * 17,
        out_specs=(vmem, hbm),
        scratch_shapes=[
            pltpu.VMEM((rows, width), BF16),
            pltpu.VMEM((1, width), F32),
            pltpu.VMEM(w_decay_down.shape[::-1], BF16),
            pltpu.VMEM(w_decay_up.shape, BF16),
            pltpu.VMEM((1, qk), F32),
            pltpu.VMEM((1, DV), F32),
            pltpu.VMEM((1, width), F32),
            pltpu.VMEM(routes.shape[::-1], jnp.int32),
            pltpu.VMEM(route_scores.shape[::-1], F32),
            pltpu.VMEM((2, share, vw), BF16),
            pltpu.VMEM(state.shape, F32),
            pltpu.VMEM(w_out.shape, BF16),
            pltpu.VMEM(w_gate_in.shape[1:], BF16),
            pltpu.VMEM(w_lin_in.shape[1:], BF16),
            pltpu.VMEM(w_down.shape[1:], BF16),
            pltpu.VMEM((ep // 2 + 2, rows, 2 * share), BF16),
            pltpu.VMEM((3 * chunks, rows, 2 * share), BF16),
            pltpu.VMEM((6, share, vw), BF16),
            pltpu.VMEM((chunks, 2 * rows, vw // 2), BF16),
            pltpu.VMEM((chunks, 2 * rows, vw // 2), BF16),
            pltpu.VMEM((ep, CAP * 8, lanes), BF16),
            pltpu.VMEM((ep, CAP * 8, lanes), BF16),
            pltpu.VMEM((ep, CAP * 8, lanes), BF16),
            pltpu.VMEM((ep, CAP * 8, lanes), BF16),
            pltpu.VMEM((ep // 2 * CAP, width), BF16),
            pltpu.VMEM((ep // 2 * CAP, ff), BF16),
            pltpu.VMEM((wide // 2, lanes), BF16),
            pltpu.VMEM((wide // 2, wide // 2), BF16),
            pltpu.VMEM((wide // 2, wide // 2), BF16),
            pltpu.SemaphoreType.DMA((17,)),
            pltpu.SemaphoreType.DMA((6,)),
            pltpu.SemaphoreType.DMA((6,)),
        ],
        compiler_params=pltpu.CompilerParams(
            collective_id=0, has_side_effects=True, vmem_limit_bytes=63_000_000
        ),
        name="layer",
    )(
        tokens,
        g_mix.reshape(1, width),
        w_decay_down.T,
        w_decay_up,
        decay_bias.reshape(1, qk),
        g_head.reshape(1, DV),
        g_ffn.reshape(1, width),
        routes.T,
        route_scores.T,
        state,
        w_query,
        w_key,
        w_value,
        w_out,
        w_gate_in,
        w_lin_in,
        w_down,
    )
    return pl.pallas_call(
        finish,
        out_shape=(
            jax.ShapeDtypeStruct((rows, width), BF16),
            jax.ShapeDtypeStruct(state.shape, F32),
        ),
        in_specs=[hbm] * 2,
        out_specs=(hbm, hbm),
        scratch_shapes=[
            pltpu.VMEM((rows, width), BF16),
            pltpu.VMEM(state.shape, F32),
            pltpu.SemaphoreType.DMA((rows + 1,)),
            pltpu.SemaphoreType.DMA((rows + 1,)),
        ],
        compiler_params=pltpu.CompilerParams(vmem_limit_bytes=63_000_000),
        name="finish",
    )(output, new_state)


def solution(mesh):
    shard = P(("grp", "ep"), None)
    experts = P("ep", None, None)
    return jax.shard_map(
        functools.partial(per_device, mesh.shape["ep"]),
        mesh=mesh,
        in_specs=(
            shard,
            P(("grp", "ep"), None, None, None),
            P(),
            P("ep", None),
            P("ep", None),
            P("ep", None),
            P(),
            P(),
            P(),
            P(),
            P(),
            P(),
            shard,
            shard,
            experts,
            experts,
            experts,
        ),
        out_specs=(shard, P(("grp", "ep"), None, None, None)),
        check_vma=False,
    )
```

```python
import functools

import jax
import jax.numpy as jnp
from jax import lax
from jax.experimental import pallas as pl
from jax.experimental.pallas import tpu as pltpu
from jax.sharding import PartitionSpec as P

MESH = pl.DeviceIdType.MESH
F32 = jnp.float32
BF16 = jnp.bfloat16

HEADS = 8
DK = 64
DV = 128
CAP = 2
EPS = 1e-06
TAU = 16.0
ALPHA = 1.702
LIMIT = 7.0

OFFSETS = (1, 4, 7, -2, -5, -7)
SEND_ORDER = (2, 5, 4, 1, 3, 0)


def rms(values, gain):
    return values * lax.rsqrt(jnp.mean(values * values, axis=-1, keepdims=True) + EPS) * gain


def dot(a, b, dims=None, precision=None):
    dims = dims or (((1,), (0,)), ((), ()))
    return lax.dot_general(a, b, dims, precision=precision, preferred_element_type=F32)


def iota(shape, dim):
    return lax.broadcasted_iota(jnp.int32, shape, dim)


def kernel(
    ep,
    tokens_in,
    g_mix_in,
    w_dd_in,
    w_du_in,
    d_bias_in,
    g_head_in,
    g_ffn_in,
    routes_in,
    scores_in,
    state,
    w_q,
    w_k,
    w_v,
    w_out,
    w_gate,
    w_lin,
    w_down,
    out,
    state_out,
    tokens,
    g_mix,
    w_dd,
    w_du,
    d_bias,
    g_head,
    g_ffn,
    routes,
    scores,
    own_w,
    st,
    wo,
    wg,
    wl,
    wd,
    xs,
    xbuf,
    wbuf,
    psend,
    rbuf,
    dsend,
    drecv,
    rsend,
    rrecv,
    st_hi,
    st_lo,
    xin,
    hid,
    acc,
    relay,
    perm,
    perm_t,
    load_sems,
    send_sems,
    recv_sems,
):
    rows, width = tokens.shape
    chips = ep // 2
    me = lax.axis_index("ep")
    z, core = me // 2, lax.rem(me, 2)

    def wrap(i):
        return lax.rem(i + 2 * chips, chips)

    def dev(zz, cc):
        return {"ep": wrap(zz) * 2 + cc}

    half = w_q.shape[1]
    pairs = [
        (tokens_in, tokens),
        (g_mix_in, g_mix),
        (w_q, own_w.at[0, :, pl.ds(0, half)]),
        (w_k, own_w.at[0, :, pl.ds(half, half)]),
        (w_v, own_w.at[1]),
        (w_dd_in, w_dd),
        (w_du_in, w_du),
        (d_bias_in, d_bias),
        (routes_in, routes),
        (scores_in, scores),
        (g_head_in, g_head),
        (g_ffn_in, g_ffn),
        (state, st),
        (w_out, wo),
        (w_gate.at[0], wg),
        (w_lin.at[0], wl),
        (w_down.at[0], wd),
    ]
    loads = [
        pltpu.make_async_copy(src, dst, load_sems.at[i]) for i, (src, dst) in enumerate(pairs)
    ]
    for c in loads[:5]:
        c.start()

    barrier = pltpu.get_barrier_semaphore()

    hops = sorted({abs(o) for o in OFFSETS}, reverse=True)
    peers = [dev(z + o * g, c) for o in hops for g in (1, -1) for c in range(2)]
    peers.append(dev(z, 1 - core))

    with jax.named_scope("hello"):
        for to in peers:
            pl.semaphore_signal(barrier, inc=1, device_id=to, device_id_type=MESH)
        for c in loads[5:]:
            c.start()
        for c in loads[:2]:
            c.wait()

    tok = tokens[...].astype(F32)
    normed = rms(tok, g_mix[...]).astype(BF16)
    for i in range(chips + 2):
        j = (i - 1) % chips
        xs[i] = normed[:, 128 * j : 128 * (j + 1)]

    for c in loads[2:5]:
        c.wait()

    with jax.named_scope("barrier"):
        pl.semaphore_wait(barrier, len(peers))

    def copy(src, dst, phase, device):
        return pltpu.make_async_remote_copy(
            src_ref=src,
            dst_ref=dst,
            send_sem=send_sems.at[phase],
            recv_sem=recv_sems.at[phase],
            device_id=device,
            device_id_type=MESH,
        )

    for oi in SEND_ORDER:
        for cc in range(2):
            zz = wrap(z + (1 - 2 * cc) * OFFSETS[oi])
            slot = 3 * (2 * oi + core)
            if oi == len(OFFSETS) - 1:
                src, dst = xs.at[pl.ds(zz + 1, 1)], xbuf.at[pl.ds(slot + 1, 1)]
            else:
                src, dst = xs.at[pl.ds(zz, 3)], xbuf.at[pl.ds(slot, 3)]
            copy(src, dst, 0, dev(zz, cc)).start()
    for n in (1, -1):
        for cc in range(2):
            copy(own_w.at[cc], wbuf.at[2 * (1 - n) + core], 1, dev(z + n, cc)).start()
    copy(own_w.at[1 - core], wbuf.at[2 + core], 1, dev(z, 1 - core)).start()

    wbuf[2 + core] = own_w[core]
    for cc in range(2):
        empty = jnp.zeros(xbuf.shape[1:], BF16)
        xbuf[3 * (10 + cc)] = empty
        xbuf[3 * (10 + cc) + 2] = empty

    for c in loads[5:12]:
        c.wait()
    low_rank = dot(normed, w_dd[...], (((1,), (1,)), ((), ()))).astype(BF16)
    pre = dot(low_rank, w_du[...]) + d_bias[...]
    log_decay = (jnp.minimum(pre, 0.0) - jnp.log1p(jnp.exp(-jnp.abs(pre)))) / TAU
    decay = jnp.exp(log_decay)

    kbs = 8
    tall = kbs * rows
    wide = ep * CAP * kbs
    r_t = lax.rem(iota((tall, rows), 0), rows)
    spread = (r_t == iota((tall, rows), 1)).astype(F32)
    route_rows = dot(
        spread, routes[...].astype(F32), (((1,), (1,)), ((), ())), lax.Precision.HIGHEST
    )
    sc = scores[...]
    e_sc = jnp.exp(sc - jnp.max(sc, axis=0, keepdims=True))
    weights = e_sc / jnp.sum(e_sc, axis=0, keepdims=True)
    weight_rows = dot(spread, weights, (((1,), (1,)), ((), ())), lax.Precision.HIGHEST)
    col = iota((tall, wide), 1)
    row = iota((tall, wide), 0)
    col_e = (col // (CAP * kbs)).astype(F32)
    col_slot = (lax.rem(col, CAP * kbs) // kbs).astype(F32)
    has = jnp.zeros((tall, wide), F32)
    weighted = jnp.zeros((tall, wide), F32)
    for j in range(routes.shape[0]):
        hit = (route_rows[:, j : j + 1] == col_e).astype(F32)
        has += hit
        weighted += hit * weight_rows[:, j : j + 1]
    rr, rc = iota((tall, tall), 0), iota((tall, tall), 1)
    before = (rr // rows == rc // rows) & (rc < rr)
    rank = dot(before.astype(BF16), has.astype(BF16))
    pick = has * (rank == col_slot).astype(F32) * (row // rows == lax.rem(col, kbs)).astype(F32)
    combine = weighted * pick
    combine_hi = combine.astype(BF16)
    combine_lo = (combine - combine_hi.astype(F32)).astype(BF16)
    pick = pick.astype(BF16)

    slots = ep * CAP
    p_r, p_c = iota((wide, wide), 0), iota((wide, wide), 1)
    perm[...] = (p_c == (lax.rem(p_r, slots) * kbs + p_r // slots)).astype(F32).astype(BF16)
    perm_t[...] = (p_r == (lax.rem(p_c, slots) * kbs + p_c // slots)).astype(F32).astype(BF16)

    loads[12].wait()
    for h in range(HEADS):
        s_h = st[:, h].reshape(rows * DK, DV)
        high = s_h.astype(BF16)
        st_hi[h] = high
        st_lo[h] = (s_h - high.astype(F32)).astype(BF16)

    chunks = 2 * len(OFFSETS)
    units = 3 * (chunks - 2) + 2
    with jax.named_scope("tokens_wait"):
        pltpu.make_async_copy(
            xbuf.at[pl.ds(0, units)], xbuf.at[pl.ds(0, units)], recv_sems.at[0]
        ).wait()
    with jax.named_scope("weights_wait"):
        pltpu.make_async_copy(
            wbuf.at[pl.ds(0, 5)], wbuf.at[pl.ds(0, 5)], recv_sems.at[1]
        ).wait()
    cols = wbuf.shape[2]
    part = None
    for n in range(3):
        x = jnp.concatenate(
            [xbuf[3 * i + n].astype(F32) for i in range(chunks)], axis=0
        ).astype(BF16)
        w = wbuf[2 * n : 2 * n + 2].reshape(2 * wbuf.shape[1], cols)
        p = dot(x, w)
        part = p if part is None else part + p
    for i in range(chunks):
        one = part[rows * i : rows * (i + 1)]
        psend[i] = jnp.concatenate(
            [one[:, : cols // 2], one[:, cols // 2 :]], axis=0
        ).astype(BF16)
    sign = 1 - 2 * core
    for oi in SEND_ORDER:
        for cc in range(2):
            to = dev(z - sign * OFFSETS[oi], cc)
            copy(psend.at[2 * oi + cc], rbuf.at[2 * oi + core], 2, to).start()
    with jax.named_scope("partials_wait"):
        pltpu.make_async_copy(
            psend, rbuf, recv_sems.at[2]
        ).wait()

    sums = []
    for h in range(2):
        total = rbuf[h].astype(F32)
        for oi in range(1, len(OFFSETS)):
            total += rbuf[2 * oi + h].astype(F32)
        sums.append(total)
    queries = sums[0][:rows] * DK ** (-0.5)
    keys = sums[0][rows:]
    values = jnp.concatenate([sums[1][:rows], sums[1][rows:]], axis=1)

    qd = queries * decay
    qk = queries * keys
    block = iota((rows, rows * DK), 1) // DK == iota((rows, rows * DK), 0)
    gain = g_head[...]
    headed = []
    for h in range(HEADS):
        q_h = qd[:, DK * h : DK * (h + 1)]
        lhs = jnp.where(block, jnp.concatenate([q_h] * rows, axis=1), 0.0)
        lhs_hi = lhs.astype(BF16)
        lhs_lo = (lhs - lhs_hi.astype(F32)).astype(BF16)
        both = dot(jnp.concatenate([lhs_hi, lhs_lo], axis=0), st_hi[h])
        a_h = both[:rows] + both[rows:] + dot(lhs_hi, st_lo[h])
        a_h += jnp.sum(qk[:, DK * h : DK * (h + 1)], axis=1, keepdims=True) * values[
            :, DV * h : DV * (h + 1)
        ]
        headed.append(rms(a_h, gain).astype(BF16))
    headed = jnp.concatenate(headed, axis=1)

    loads[13].wait()
    residual = (tok + dot(headed, wo[...])).astype(BF16).astype(F32)
    fed = rms(residual, g_ffn[...])

    lanes = width // (2 * kbs)
    mid = width // 2
    fed_rows = jnp.concatenate(
        [
            jnp.concatenate(
                [fed[:, mid * b + lanes * k : mid * b + lanes * (k + 1)] for b in range(2)],
                axis=1,
            )
            for k in range(kbs)
        ],
        axis=0,
    ).astype(BF16)
    picked = dot(pick, fed_rows, (((0,), (0,)), ((), ())))
    for b in range(2):
        dsend[b] = picked[:, lanes * b : lanes * (b + 1)].astype(BF16).reshape(dsend.shape[1:])

    quarter = chips // 4
    far_side = range(chips // 2 - 1, quarter, -1)
    near_side = range(quarter, 0, -1)

    def ring_send(src, dst, phase, o):
        for cc in range(2):
            there = wrap(z + o) * 2 + cc
            copy(src.at[there], dst.at[me], phase, {"ep": there}).start()

    def send_up(src, dst, phase):
        there = wrap(z + chips // 2) * 2
        copy(src.at[there], dst.at[me], phase, {"ep": there}).start()
        for o in range(chips // 2 - 1, 0, -1):
            ring_send(src, dst, phase, o)
        there = 2 * z + 1 - core
        copy(src.at[there], dst.at[me], phase, {"ep": there}).start()
        dst[me] = src[me]

    def send_relay(src, via, phase):
        there = wrap(z + chips // 2) * 2 + 1
        copy(src.at[there], via, phase, dev(z - quarter, core)).start()

    def send_down(src, dst, phase, side):
        for o in side:
            ring_send(src, dst, phase, -o)

    def forward(via, relay_phase, dst, phase):
        pltpu.make_async_copy(via, via, recv_sems.at[relay_phase]).wait()
        origin = wrap(z + quarter) * 2 + core
        copy(via, dst.at[origin], phase, dev(z - quarter, 1)).start()

    def arrive(src, dst, phase):
        pltpu.make_async_copy(
            src.at[pl.ds(0, ep - 1)], dst.at[pl.ds(0, ep - 1)], recv_sems.at[phase]
        ).wait()

    with jax.named_scope("dispatch"):
        for b in range(2):
            send_relay(dsend.at[b], relay.at[b], 7 + b)
            send_up(dsend.at[b], drecv.at[b], 3 + b)
            if b == 0:
                send_down(dsend.at[b], drecv.at[b], 3 + b, far_side)

    with jax.named_scope("new_state"):
        decay_cols, key_cols = decay.T, keys.T
        for t in range(rows):
            for h in range(HEADS):
                at = slice(DK * h, DK * (h + 1))
                st[t, h] = (
                    decay_cols[at, t : t + 1] * st[t, h]
                    + key_cols[at, t : t + 1] * values[t : t + 1, DV * h : DV * (h + 1)]
                )
        store = pltpu.make_async_copy(st, state_out, load_sems.at[12])
        store.start()

    with jax.named_scope("dispatch_relay"):
        forward(relay.at[0], 7, drecv.at[0], 3)
        send_down(dsend.at[0], drecv.at[0], 3, near_side)
        send_down(dsend.at[1], drecv.at[1], 4, far_side)
        forward(relay.at[1], 8, drecv.at[1], 4)
        send_down(dsend.at[1], drecv.at[1], 4, near_side)

    tile = 256

    def up(b):
        half_in = slice(mid * b, mid * (b + 1))
        arrived = dot(perm[...], drecv[b].reshape(wide, lanes)).astype(BF16)
        for k in range(kbs):
            xin[:, mid * b + lanes * k : mid * b + lanes * (k + 1)] = arrived[
                slots * k : slots * (k + 1)
            ]

        def step(i, carry):
            cols = pl.ds(pl.multiple_of(i * tile, tile), tile)
            x = xin[:, half_in]
            gate, lin = dot(x, wg[half_in, cols]), dot(x, wl[half_in, cols])
            if b == 0:
                acc[0, :, cols] = gate
                acc[1, :, cols] = lin
            else:
                gate = jnp.minimum(gate + acc[0, :, cols], LIMIT)
                lin = jnp.clip(lin + acc[1, :, cols], -LIMIT, LIMIT)
                hid[:, cols] = (gate * jax.nn.sigmoid(ALPHA * gate) * (lin + 1.0)).astype(BF16)
            return carry

        lax.fori_loop(0, wg.shape[1] // tile, step, 0)

    def down(b):
        blocks = []
        for at in range(mid * b, mid * (b + 1), tile):
            both = dot(hid[...], wd[:, at : at + tile])
            blocks += [both[:, lanes * k : lanes * (k + 1)] for k in range(tile // lanes)]
        expert_out = jnp.concatenate(blocks, axis=0).astype(BF16)
        rsend[b] = dot(perm_t[...], expert_out).astype(BF16).reshape(rsend.shape[1:])

    with jax.named_scope("half_wait"):
        arrive(dsend.at[0], drecv.at[0], 3)
    for c in loads[14:]:
        c.wait()
    with jax.named_scope("half_up"):
        up(0)
    with jax.named_scope("full_wait"):
        arrive(dsend.at[1], drecv.at[1], 4)
    with jax.named_scope("full_up"):
        up(1)
    with jax.named_scope("down"):
        down(0)
    with jax.named_scope("half_back"):
        send_relay(rsend.at[0], relay.at[2], 9)
        send_up(rsend.at[0], rrecv.at[0], 5)
        send_down(rsend.at[0], rrecv.at[0], 5, far_side)
    with jax.named_scope("down_rest"):
        down(1)
    with jax.named_scope("full_back"):
        send_relay(rsend.at[1], relay.at[3], 10)
        send_up(rsend.at[1], rrecv.at[1], 6)
        forward(relay.at[2], 9, rrecv.at[0], 5)
        send_down(rsend.at[0], rrecv.at[0], 5, near_side)
        send_down(rsend.at[1], rrecv.at[1], 6, far_side)
        forward(relay.at[3], 10, rrecv.at[1], 6)
        send_down(rsend.at[1], rrecv.at[1], 6, near_side)

    for b in range(2):
        with jax.named_scope("back_wait"):
            arrive(rsend.at[b], rrecv.at[b], 5 + b)
        back = rrecv[b].reshape(wide, lanes)
        mixed = dot(combine_hi, back) + dot(combine_lo, back)
        for k in range(kbs):
            at = slice(mid * b + lanes * k, mid * b + lanes * (k + 1))
            out[:, at] = (residual[:, at] + mixed[rows * k : rows * (k + 1)]).astype(BF16)

    store.wait()
    pltpu.make_async_copy(
        xbuf.at[pl.ds(0, units)], xbuf.at[pl.ds(0, units)], send_sems.at[0]
    ).wait()
    pltpu.make_async_copy(wbuf.at[pl.ds(0, 5)], wbuf.at[pl.ds(0, 5)], send_sems.at[1]).wait()
    pltpu.make_async_copy(psend, rbuf, send_sems.at[2]).wait()
    for b in range(2):
        for src, dst, phase in ((dsend, drecv, 3), (rsend, rrecv, 5)):
            pltpu.make_async_copy(
                src.at[b, pl.ds(0, ep - 1)], dst.at[b, pl.ds(0, ep - 1)], send_sems.at[phase + b]
            ).wait()
        for i in (b, 2 + b):
            pltpu.make_async_copy(relay.at[i], relay.at[i], send_sems.at[7 + i]).wait()


def finish(out_in, state_in, out, state_out, out_buf, state_buf, in_sems, out_sems):
    rows = state_in.shape[0]
    ways = [(state_in.at[i], state_buf.at[i], state_out.at[i]) for i in range(rows)]
    ways.append((out_in, out_buf, out))
    ins = [pltpu.make_async_copy(w[0], w[1], in_sems.at[i]) for i, w in enumerate(ways)]
    outs = [pltpu.make_async_copy(w[1], w[2], out_sems.at[i]) for i, w in enumerate(ways)]
    for c in ins:
        c.start()
    for c, d in zip(ins, outs):
        c.wait()
        d.start()
    for d in outs:
        d.wait()


def per_device(
    ep,
    tokens,
    state,
    g_mix,
    w_query,
    w_key,
    w_value,
    w_decay_down,
    w_decay_up,
    decay_bias,
    g_head,
    w_out,
    g_ffn,
    routes,
    route_scores,
    w_gate_in,
    w_lin_in,
    w_down,
):
    rows, width = tokens.shape
    share, qk = w_query.shape
    vw = w_value.shape[1]
    ff = w_gate_in.shape[2]
    lanes = width // 16
    wide = ep * CAP * 8
    vmem = pl.BlockSpec(memory_space=pltpu.VMEM)
    hbm = pl.BlockSpec(memory_space=pltpu.HBM)
    chunks = 2 * len(OFFSETS)
    output, new_state = pl.pallas_call(
        functools.partial(kernel, ep),
        out_shape=(
            jax.ShapeDtypeStruct((rows, width), BF16),
            jax.ShapeDtypeStruct(state.shape, F32),
        ),
        in_specs=[hbm] * 17,
        out_specs=(vmem, hbm),
        scratch_shapes=[
            pltpu.VMEM((rows, width), BF16),
            pltpu.VMEM((1, width), F32),
            pltpu.VMEM(w_decay_down.shape[::-1], BF16),
            pltpu.VMEM(w_decay_up.shape, BF16),
            pltpu.VMEM((1, qk), F32),
            pltpu.VMEM((1, DV), F32),
            pltpu.VMEM((1, width), F32),
            pltpu.VMEM(routes.shape[::-1], jnp.int32),
            pltpu.VMEM(route_scores.shape[::-1], F32),
            pltpu.VMEM((2, share, vw), BF16),
            pltpu.VMEM(state.shape, F32),
            pltpu.VMEM(w_out.shape, BF16),
            pltpu.VMEM(w_gate_in.shape[1:], BF16),
            pltpu.VMEM(w_lin_in.shape[1:], BF16),
            pltpu.VMEM(w_down.shape[1:], BF16),
            pltpu.VMEM((ep // 2 + 2, rows, 2 * share), BF16),
            pltpu.VMEM((3 * chunks, rows, 2 * share), BF16),
            pltpu.VMEM((6, share, vw), BF16),
            pltpu.VMEM((chunks, 2 * rows, vw // 2), BF16),
            pltpu.VMEM((chunks, 2 * rows, vw // 2), BF16),
            pltpu.VMEM((2, ep, CAP * 8, lanes), BF16),
            pltpu.VMEM((2, ep, CAP * 8, lanes), BF16),
            pltpu.VMEM((2, ep, CAP * 8, lanes), BF16),
            pltpu.VMEM((2, ep, CAP * 8, lanes), BF16),
            pltpu.VMEM((HEADS, rows * DK, DV), BF16),
            pltpu.VMEM((HEADS, rows * DK, DV), BF16),
            pltpu.VMEM((ep * CAP, width), BF16),
            pltpu.VMEM((ep * CAP, ff), BF16),
            pltpu.VMEM((2, ep * CAP, ff), F32),
            pltpu.VMEM((4, CAP * 8, lanes), BF16),
            pltpu.VMEM((wide, wide), BF16),
            pltpu.VMEM((wide, wide), BF16),
            pltpu.SemaphoreType.DMA((17,)),
            pltpu.SemaphoreType.DMA((11,)),
            pltpu.SemaphoreType.DMA((11,)),
        ],
        compiler_params=pltpu.CompilerParams(
            collective_id=0, has_side_effects=True, vmem_limit_bytes=63_000_000
        ),
        name="layer",
    )(
        tokens,
        g_mix.reshape(1, width),
        w_decay_down.T,
        w_decay_up,
        decay_bias.reshape(1, qk),
        g_head.reshape(1, DV),
        g_ffn.reshape(1, width),
        routes.T,
        route_scores.T,
        state,
        w_query,
        w_key,
        w_value,
        w_out,
        w_gate_in,
        w_lin_in,
        w_down,
    )
    return pl.pallas_call(
        finish,
        out_shape=(
            jax.ShapeDtypeStruct((rows, width), BF16),
            jax.ShapeDtypeStruct(state.shape, F32),
        ),
        in_specs=[hbm] * 2,
        out_specs=(hbm, hbm),
        scratch_shapes=[
            pltpu.VMEM((rows, width), BF16),
            pltpu.VMEM(state.shape, F32),
            pltpu.SemaphoreType.DMA((rows + 1,)),
            pltpu.SemaphoreType.DMA((rows + 1,)),
        ],
        compiler_params=pltpu.CompilerParams(vmem_limit_bytes=63_000_000),
        name="finish",
    )(output, new_state)


def solution(mesh):
    shard = P(("grp", "ep"), None)
    experts = P("ep", None, None)
    return jax.shard_map(
        functools.partial(per_device, mesh.shape["ep"]),
        mesh=mesh,
        in_specs=(
            shard,
            P(("grp", "ep"), None, None, None),
            P(),
            P("ep", None),
            P("ep", None),
            P("ep", None),
            P(),
            P(),
            P(),
            P(),
            P(),
            P(),
            shard,
            shard,
            experts,
            experts,
            experts,
        ),
        out_specs=(shard, P(("grp", "ep"), None, None, None)),
        check_vma=False,
    )
```

```python
import functools

import jax
import jax.numpy as jnp
from jax import lax
from jax.experimental import pallas as pl
from jax.experimental.pallas import tpu as pltpu
from jax.sharding import PartitionSpec as P

MESH = pl.DeviceIdType.MESH
F32 = jnp.float32
BF16 = jnp.bfloat16

HEADS = 8
DK = 64
DV = 128
CAP = 2
EPS = 1e-06
TAU = 16.0
ALPHA = 1.702
LIMIT = 7.0

OFFSETS = (1, 4, 7, -2, -5, -7)
SEND_ORDER = (2, 5, 4, 1, 3, 0)


def rms(values, gain):
    return values * lax.rsqrt(jnp.mean(values * values, axis=-1, keepdims=True) + EPS) * gain


def dot(a, b, dims=None, precision=None):
    dims = dims or (((1,), (0,)), ((), ()))
    return lax.dot_general(a, b, dims, precision=precision, preferred_element_type=F32)


def iota(shape, dim):
    return lax.broadcasted_iota(jnp.int32, shape, dim)


def kernel(
    ep,
    tokens_in,
    g_mix_in,
    w_dd_in,
    w_du_in,
    d_bias_in,
    g_head_in,
    g_ffn_in,
    routes_in,
    scores_in,
    state,
    w_q,
    w_k,
    w_v,
    w_out,
    w_gate,
    w_lin,
    w_down,
    out,
    state_out,
    tokens,
    g_mix,
    w_dd,
    w_du,
    d_bias,
    g_head,
    g_ffn,
    routes,
    scores,
    own_w,
    st,
    wo,
    wg,
    wl,
    wd,
    xs,
    xbuf,
    wbuf,
    psend,
    rbuf,
    dsend,
    drecv,
    rsend,
    rrecv,
    st_hi,
    st_lo,
    xin,
    hid,
    perm,
    perm_t,
    load_sems,
    send_sems,
    recv_sems,
):
    rows, width = tokens.shape
    chips = ep // 2
    me = lax.axis_index("ep")
    z, core = me // 2, lax.rem(me, 2)

    def wrap(i):
        return lax.rem(i + 2 * chips, chips)

    def dev(zz, cc):
        return {"ep": wrap(zz) * 2 + cc}

    half = w_q.shape[1]
    pairs = [
        (tokens_in, tokens),
        (g_mix_in, g_mix),
        (w_q, own_w.at[0, :, pl.ds(0, half)]),
        (w_k, own_w.at[0, :, pl.ds(half, half)]),
        (w_v, own_w.at[1]),
        (w_dd_in, w_dd),
        (w_du_in, w_du),
        (d_bias_in, d_bias),
        (routes_in, routes),
        (scores_in, scores),
        (g_head_in, g_head),
        (g_ffn_in, g_ffn),
        (state, st),
        (w_out, wo),
        (w_gate.at[0], wg),
        (w_lin.at[0], wl),
        (w_down.at[0], wd),
    ]
    loads = [
        pltpu.make_async_copy(src, dst, load_sems.at[i]) for i, (src, dst) in enumerate(pairs)
    ]
    for c in loads[:5]:
        c.start()

    barrier = pltpu.get_barrier_semaphore()

    hops = sorted({abs(o) for o in OFFSETS}, reverse=True)
    peers = [dev(z + o * g, c) for o in hops for g in (1, -1) for c in range(2)]
    peers.append(dev(z, 1 - core))

    with jax.named_scope("hello"):
        for to in peers:
            pl.semaphore_signal(barrier, inc=1, device_id=to, device_id_type=MESH)
        for c in loads[5:]:
            c.start()
        for c in loads[:2]:
            c.wait()

    tok = tokens[...].astype(F32)
    normed = rms(tok, g_mix[...]).astype(BF16)
    for i in range(chips + 2):
        j = (i - 1) % chips
        xs[i] = normed[:, 128 * j : 128 * (j + 1)]

    for c in loads[2:5]:
        c.wait()

    with jax.named_scope("barrier"):
        pl.semaphore_wait(barrier, len(peers))

    def copy(src, dst, phase, device):
        return pltpu.make_async_remote_copy(
            src_ref=src,
            dst_ref=dst,
            send_sem=send_sems.at[phase],
            recv_sem=recv_sems.at[phase],
            device_id=device,
            device_id_type=MESH,
        )

    for cc in range(2):
        for oi in SEND_ORDER:
            zz = wrap(z + (1 - 2 * cc) * OFFSETS[oi])
            slot = 3 * (2 * oi + core)
            if oi == len(OFFSETS) - 1:
                src, dst = xs.at[pl.ds(zz + 1, 1)], xbuf.at[pl.ds(slot + 1, 1)]
            else:
                src, dst = xs.at[pl.ds(zz, 3)], xbuf.at[pl.ds(slot, 3)]
            copy(src, dst, 0, dev(zz, cc)).start()
        for n in (1, -1):
            copy(own_w.at[cc], wbuf.at[2 * (1 - n) + core], 1, dev(z + n, cc)).start()
    copy(own_w.at[1 - core], wbuf.at[2 + core], 1, dev(z, 1 - core)).start()

    wbuf[2 + core] = own_w[core]
    for cc in range(2):
        empty = jnp.zeros(xbuf.shape[1:], BF16)
        xbuf[3 * (10 + cc)] = empty
        xbuf[3 * (10 + cc) + 2] = empty

    for c in loads[5:12]:
        c.wait()
    low_rank = dot(normed, w_dd[...], (((1,), (1,)), ((), ()))).astype(BF16)
    pre = dot(low_rank, w_du[...]) + d_bias[...]
    log_decay = (jnp.minimum(pre, 0.0) - jnp.log1p(jnp.exp(-jnp.abs(pre)))) / TAU
    decay = jnp.exp(log_decay)

    kbs = 8
    tall = kbs * rows
    wide = ep * CAP * kbs
    r_t = lax.rem(iota((tall, rows), 0), rows)
    spread = (r_t == iota((tall, rows), 1)).astype(F32)
    route_rows = dot(
        spread, routes[...].astype(F32), (((1,), (1,)), ((), ())), lax.Precision.HIGHEST
    )
    sc = scores[...]
    e_sc = jnp.exp(sc - jnp.max(sc, axis=0, keepdims=True))
    weights = e_sc / jnp.sum(e_sc, axis=0, keepdims=True)
    weight_rows = dot(spread, weights, (((1,), (1,)), ((), ())), lax.Precision.HIGHEST)
    col = iota((tall, wide), 1)
    row = iota((tall, wide), 0)
    col_e = (col // (CAP * kbs)).astype(F32)
    col_slot = (lax.rem(col, CAP * kbs) // kbs).astype(F32)
    has = jnp.zeros((tall, wide), F32)
    weighted = jnp.zeros((tall, wide), F32)
    for j in range(routes.shape[0]):
        hit = (route_rows[:, j : j + 1] == col_e).astype(F32)
        has += hit
        weighted += hit * weight_rows[:, j : j + 1]
    rr, rc = iota((tall, tall), 0), iota((tall, tall), 1)
    before = (rr // rows == rc // rows) & (rc < rr)
    rank = dot(before.astype(BF16), has.astype(BF16))
    pick = has * (rank == col_slot).astype(F32) * (row // rows == lax.rem(col, kbs)).astype(F32)
    combine = weighted * pick
    combine_hi = combine.astype(BF16)
    combine_lo = (combine - combine_hi.astype(F32)).astype(BF16)
    pick = pick.astype(BF16)

    slots = ep * CAP
    p_r, p_c = iota((wide, wide), 0), iota((wide, wide), 1)
    perm[...] = (p_c == (lax.rem(p_r, slots) * kbs + p_r // slots)).astype(F32).astype(BF16)
    perm_t[...] = (p_r == (lax.rem(p_c, slots) * kbs + p_c // slots)).astype(F32).astype(BF16)

    loads[12].wait()
    for h in range(HEADS):
        s_h = st[:, h].reshape(rows * DK, DV)
        high = s_h.astype(BF16)
        st_hi[h] = high
        st_lo[h] = (s_h - high.astype(F32)).astype(BF16)

    chunks = 2 * len(OFFSETS)
    units = 3 * (chunks - 2) + 2
    with jax.named_scope("tokens_wait"):
        pltpu.make_async_copy(
            xbuf.at[pl.ds(0, units)], xbuf.at[pl.ds(0, units)], recv_sems.at[0]
        ).wait()
    with jax.named_scope("weights_wait"):
        pltpu.make_async_copy(
            wbuf.at[pl.ds(0, 5)], wbuf.at[pl.ds(0, 5)], recv_sems.at[1]
        ).wait()
    cols = wbuf.shape[2]
    part = None
    for n in range(3):
        x = jnp.concatenate(
            [xbuf[3 * i + n].astype(F32) for i in range(chunks)], axis=0
        ).astype(BF16)
        w = wbuf[2 * n : 2 * n + 2].reshape(2 * wbuf.shape[1], cols)
        p = dot(x, w)
        part = p if part is None else part + p
    for i in range(chunks):
        one = part[rows * i : rows * (i + 1)]
        psend[i] = jnp.concatenate(
            [one[:, : cols // 2], one[:, cols // 2 :]], axis=0
        ).astype(BF16)
    sign = 1 - 2 * core
    for cc in range(2):
        for oi in SEND_ORDER:
            to = dev(z - sign * OFFSETS[oi], cc)
            copy(psend.at[2 * oi + cc], rbuf.at[2 * oi + core], 2, to).start()
    with jax.named_scope("partials_wait"):
        pltpu.make_async_copy(
            psend, rbuf, recv_sems.at[2]
        ).wait()

    sums = []
    for h in range(2):
        total = rbuf[h].astype(F32)
        for oi in range(1, len(OFFSETS)):
            total += rbuf[2 * oi + h].astype(F32)
        sums.append(total)
    queries = sums[0][:rows] * DK ** (-0.5)
    keys = sums[0][rows:]
    values = jnp.concatenate([sums[1][:rows], sums[1][rows:]], axis=1)

    qd = queries * decay
    qk = queries * keys
    block = iota((rows, rows * DK), 1) // DK == iota((rows, rows * DK), 0)
    gain = g_head[...]
    headed = []
    for h in range(HEADS):
        q_h = qd[:, DK * h : DK * (h + 1)]
        lhs = jnp.where(block, jnp.concatenate([q_h] * rows, axis=1), 0.0)
        lhs_hi = lhs.astype(BF16)
        lhs_lo = (lhs - lhs_hi.astype(F32)).astype(BF16)
        both = dot(jnp.concatenate([lhs_hi, lhs_lo], axis=0), st_hi[h])
        a_h = both[:rows] + both[rows:] + dot(lhs_hi, st_lo[h])
        a_h += jnp.sum(qk[:, DK * h : DK * (h + 1)], axis=1, keepdims=True) * values[
            :, DV * h : DV * (h + 1)
        ]
        headed.append(rms(a_h, gain).astype(BF16))
    headed = jnp.concatenate(headed, axis=1)

    loads[13].wait()
    residual = (tok + dot(headed, wo[...])).astype(BF16).astype(F32)
    fed = rms(residual, g_ffn[...])

    lanes = width // kbs
    fed_rows = jnp.concatenate(
        [fed[:, lanes * k : lanes * (k + 1)] for k in range(kbs)], axis=0
    ).astype(BF16)
    dsend[...] = (
        dot(pick, fed_rows, (((0,), (0,)), ((), ()))).astype(BF16).reshape(dsend.shape)
    )

    def exchange(src, dst, phase):
        for cc in range(2):
            for o in range(chips // 2, 0, -1):
                for oo in (o, -o)[: 1 + (o < chips // 2)]:
                    there = wrap(z + oo) * 2 + cc
                    copy(src.at[there], dst.at[me], phase, {"ep": there}).start()
        there = 2 * z + 1 - core
        copy(src.at[there], dst.at[me], phase, {"ep": there}).start()
        dst[me] = src[me]

    def arrive(src, dst, phase):
        pltpu.make_async_copy(
            src.at[pl.ds(0, ep - 1)], dst.at[pl.ds(0, ep - 1)], recv_sems.at[phase]
        ).wait()

    with jax.named_scope("dispatch"):
        exchange(dsend, drecv, 3)

    with jax.named_scope("new_state"):
        decay_cols, key_cols = decay.T, keys.T
        for t in range(rows):
            for h in range(HEADS):
                at = slice(DK * h, DK * (h + 1))
                st[t, h] = (
                    decay_cols[at, t : t + 1] * st[t, h]
                    + key_cols[at, t : t + 1] * values[t : t + 1, DV * h : DV * (h + 1)]
                )
        store = pltpu.make_async_copy(st, state_out, load_sems.at[12])
        store.start()

    with jax.named_scope("dispatch_wait"):
        arrive(dsend, drecv, 3)
    with jax.named_scope("expert"):
        arrived = dot(perm[...], drecv[...].reshape(wide, lanes)).astype(BF16)
        for k in range(kbs):
            xin[:, lanes * k : lanes * (k + 1)] = arrived[slots * k : slots * (k + 1)]
        for c in loads[14:]:
            c.wait()
        tile = 256

        def up(i, carry):
            cols = pl.ds(pl.multiple_of(i * tile, tile), tile)
            x = xin[...]
            gate = jnp.minimum(dot(x, wg[:, cols]), LIMIT)
            lin = jnp.clip(dot(x, wl[:, cols]), -LIMIT, LIMIT)
            hid[:, cols] = (gate * jax.nn.sigmoid(ALPHA * gate) * (lin + 1.0)).astype(BF16)
            return carry

        lax.fori_loop(0, wg.shape[1] // tile, up, 0)
        expert_out = jnp.concatenate(
            [dot(hid[...], wd[:, lanes * k : lanes * (k + 1)]) for k in range(kbs)], axis=0
        ).astype(BF16)
        rsend[...] = dot(perm_t[...], expert_out).astype(BF16).reshape(rsend.shape)
    with jax.named_scope("back"):
        exchange(rsend, rrecv, 4)
    with jax.named_scope("back_wait"):
        arrive(rsend, rrecv, 4)

    back = rrecv[...].reshape(wide, lanes)
    mixed = dot(combine_hi, back) + dot(combine_lo, back)
    for k in range(kbs):
        at = slice(lanes * k, lanes * (k + 1))
        out[:, at] = (residual[:, at] + mixed[rows * k : rows * (k + 1)]).astype(BF16)

    store.wait()
    pltpu.make_async_copy(
        xbuf.at[pl.ds(0, units)], xbuf.at[pl.ds(0, units)], send_sems.at[0]
    ).wait()
    pltpu.make_async_copy(wbuf.at[pl.ds(0, 5)], wbuf.at[pl.ds(0, 5)], send_sems.at[1]).wait()
    pltpu.make_async_copy(psend, rbuf, send_sems.at[2]).wait()
    for src, dst, phase in ((dsend, drecv, 3), (rsend, rrecv, 4)):
        pltpu.make_async_copy(
            src.at[pl.ds(0, ep - 1)], dst.at[pl.ds(0, ep - 1)], send_sems.at[phase]
        ).wait()


def finish(out_in, state_in, out, state_out, out_buf, state_buf, in_sems, out_sems):
    rows = state_in.shape[0]
    ways = [(state_in.at[i], state_buf.at[i], state_out.at[i]) for i in range(rows)]
    ways.append((out_in, out_buf, out))
    ins = [pltpu.make_async_copy(w[0], w[1], in_sems.at[i]) for i, w in enumerate(ways)]
    outs = [pltpu.make_async_copy(w[1], w[2], out_sems.at[i]) for i, w in enumerate(ways)]
    for c in ins:
        c.start()
    for c, d in zip(ins, outs):
        c.wait()
        d.start()
    for d in outs:
        d.wait()


def per_device(
    ep,
    tokens,
    state,
    g_mix,
    w_query,
    w_key,
    w_value,
    w_decay_down,
    w_decay_up,
    decay_bias,
    g_head,
    w_out,
    g_ffn,
    routes,
    route_scores,
    w_gate_in,
    w_lin_in,
    w_down,
):
    rows, width = tokens.shape
    share, qk = w_query.shape
    vw = w_value.shape[1]
    ff = w_gate_in.shape[2]
    lanes = width // 8
    wide = ep * CAP * 8
    vmem = pl.BlockSpec(memory_space=pltpu.VMEM)
    hbm = pl.BlockSpec(memory_space=pltpu.HBM)
    chunks = 2 * len(OFFSETS)
    output, new_state = pl.pallas_call(
        functools.partial(kernel, ep),
        out_shape=(
            jax.ShapeDtypeStruct((rows, width), BF16),
            jax.ShapeDtypeStruct(state.shape, F32),
        ),
        in_specs=[hbm] * 17,
        out_specs=(vmem, hbm),
        scratch_shapes=[
            pltpu.VMEM((rows, width), BF16),
            pltpu.VMEM((1, width), F32),
            pltpu.VMEM(w_decay_down.shape[::-1], BF16),
            pltpu.VMEM(w_decay_up.shape, BF16),
            pltpu.VMEM((1, qk), F32),
            pltpu.VMEM((1, DV), F32),
            pltpu.VMEM((1, width), F32),
            pltpu.VMEM(routes.shape[::-1], jnp.int32),
            pltpu.VMEM(route_scores.shape[::-1], F32),
            pltpu.VMEM((2, share, vw), BF16),
            pltpu.VMEM(state.shape, F32),
            pltpu.VMEM(w_out.shape, BF16),
            pltpu.VMEM(w_gate_in.shape[1:], BF16),
            pltpu.VMEM(w_lin_in.shape[1:], BF16),
            pltpu.VMEM(w_down.shape[1:], BF16),
            pltpu.VMEM((ep // 2 + 2, rows, 2 * share), BF16),
            pltpu.VMEM((3 * chunks, rows, 2 * share), BF16),
            pltpu.VMEM((6, share, vw), BF16),
            pltpu.VMEM((chunks, 2 * rows, vw // 2), BF16),
            pltpu.VMEM((chunks, 2 * rows, vw // 2), BF16),
            pltpu.VMEM((ep, CAP * 8, lanes), BF16),
            pltpu.VMEM((ep, CAP * 8, lanes), BF16),
            pltpu.VMEM((ep, CAP * 8, lanes), BF16),
            pltpu.VMEM((ep, CAP * 8, lanes), BF16),
            pltpu.VMEM((HEADS, rows * DK, DV), BF16),
            pltpu.VMEM((HEADS, rows * DK, DV), BF16),
            pltpu.VMEM((ep * CAP, width), BF16),
            pltpu.VMEM((ep * CAP, ff), BF16),
            pltpu.VMEM((wide, wide), BF16),
            pltpu.VMEM((wide, wide), BF16),
            pltpu.SemaphoreType.DMA((17,)),
            pltpu.SemaphoreType.DMA((5,)),
            pltpu.SemaphoreType.DMA((5,)),
        ],
        compiler_params=pltpu.CompilerParams(
            collective_id=0, has_side_effects=True, vmem_limit_bytes=63_000_000
        ),
        name="layer",
    )(
        tokens,
        g_mix.reshape(1, width),
        w_decay_down.T,
        w_decay_up,
        decay_bias.reshape(1, qk),
        g_head.reshape(1, DV),
        g_ffn.reshape(1, width),
        routes.T,
        route_scores.T,
        state,
        w_query,
        w_key,
        w_value,
        w_out,
        w_gate_in,
        w_lin_in,
        w_down,
    )
    return pl.pallas_call(
        finish,
        out_shape=(
            jax.ShapeDtypeStruct((rows, width), BF16),
            jax.ShapeDtypeStruct(state.shape, F32),
        ),
        in_specs=[hbm] * 2,
        out_specs=(hbm, hbm),
        scratch_shapes=[
            pltpu.VMEM((rows, width), BF16),
            pltpu.VMEM(state.shape, F32),
            pltpu.SemaphoreType.DMA((rows + 1,)),
            pltpu.SemaphoreType.DMA((rows + 1,)),
        ],
        compiler_params=pltpu.CompilerParams(vmem_limit_bytes=63_000_000),
        name="finish",
    )(output, new_state)


def solution(mesh):
    shard = P(("grp", "ep"), None)
    experts = P("ep", None, None)
    return jax.shard_map(
        functools.partial(per_device, mesh.shape["ep"]),
        mesh=mesh,
        in_specs=(
            shard,
            P(("grp", "ep"), None, None, None),
            P(),
            P("ep", None),
            P("ep", None),
            P("ep", None),
            P(),
            P(),
            P(),
            P(),
            P(),
            P(),
            shard,
            shard,
            experts,
            experts,
            experts,
        ),
        out_specs=(shard, P(("grp", "ep"), None, None, None)),
        check_vma=False,
    )
```

```python
import functools

import jax
import jax.numpy as jnp
from jax import lax
from jax.experimental import pallas as pl
from jax.experimental.pallas import tpu as pltpu
from jax.sharding import PartitionSpec as P

MESH = pl.DeviceIdType.MESH
F32 = jnp.float32
BF16 = jnp.bfloat16

HEADS = 8
DK = 64
DV = 128
CAP = 2
EPS = 1e-06
TAU = 16.0
ALPHA = 1.702
LIMIT = 7.0

OFFSETS = (1, 4, 7, -2, -5, -7)
SEND_ORDER = (2, 5, 4, 1, 3, 0)


def rms(values, gain):
    return values * lax.rsqrt(jnp.mean(values * values, axis=-1, keepdims=True) + EPS) * gain


def dot(a, b, dims=None, precision=None):
    dims = dims or (((1,), (0,)), ((), ()))
    return lax.dot_general(a, b, dims, precision=precision, preferred_element_type=F32)


def iota(shape, dim):
    return lax.broadcasted_iota(jnp.int32, shape, dim)


def kernel(
    ep,
    tokens_in,
    g_mix_in,
    w_dd_in,
    w_du_in,
    d_bias_in,
    g_head_in,
    g_ffn_in,
    routes_in,
    scores_in,
    state,
    w_q,
    w_k,
    w_v,
    w_out,
    w_gate,
    w_lin,
    w_down,
    out,
    state_out,
    tokens,
    g_mix,
    w_dd,
    w_du,
    d_bias,
    g_head,
    g_ffn,
    routes,
    scores,
    own_w,
    st,
    wo,
    wg,
    wl,
    wd,
    xs,
    xbuf,
    wbuf,
    psend,
    rbuf,
    dsend,
    drecv,
    rsend,
    rrecv,
    st_hi,
    st_lo,
    xin,
    hid,
    perm,
    perm_t,
    load_sems,
    send_sems,
    recv_sems,
):
    rows, width = tokens.shape
    chips = ep // 2
    me = lax.axis_index("ep")
    z, core = me // 2, lax.rem(me, 2)

    def wrap(i):
        return lax.rem(i + 2 * chips, chips)

    def dev(zz, cc):
        return {"ep": wrap(zz) * 2 + cc}

    half = w_q.shape[1]
    pairs = [
        (tokens_in, tokens),
        (g_mix_in, g_mix),
        (w_q, own_w.at[0, :, pl.ds(0, half)]),
        (w_k, own_w.at[0, :, pl.ds(half, half)]),
        (w_v, own_w.at[1]),
        (w_dd_in, w_dd),
        (w_du_in, w_du),
        (d_bias_in, d_bias),
        (routes_in, routes),
        (scores_in, scores),
        (g_head_in, g_head),
        (g_ffn_in, g_ffn),
        (state, st),
        (w_out, wo),
        (w_gate.at[0], wg),
        (w_lin.at[0], wl),
        (w_down.at[0], wd),
    ]
    loads = [
        pltpu.make_async_copy(src, dst, load_sems.at[i]) for i, (src, dst) in enumerate(pairs)
    ]
    barrier = pltpu.get_barrier_semaphore()

    hops = sorted({abs(o) for o in OFFSETS}, reverse=True)
    peers = [dev(z + o * g, c) for o in hops for g in (1, -1) for c in range(2)]
    peers.append(dev(z, 1 - core))

    with jax.named_scope("hello"):
        for to in peers:
            pl.semaphore_signal(barrier, inc=1, device_id=to, device_id_type=MESH)
        for c in loads:
            c.start()
        for c in loads[:2]:
            c.wait()

    tok = tokens[...].astype(F32)
    normed = rms(tok, g_mix[...]).astype(BF16)
    for i in range(chips + 2):
        j = (i - 1) % chips
        xs[i] = normed[:, 128 * j : 128 * (j + 1)]

    for c in loads[2:5]:
        c.wait()

    with jax.named_scope("barrier"):
        pl.semaphore_wait(barrier, len(peers))

    def copy(src, dst, phase, device):
        return pltpu.make_async_remote_copy(
            src_ref=src,
            dst_ref=dst,
            send_sem=send_sems.at[phase],
            recv_sem=recv_sems.at[phase],
            device_id=device,
            device_id_type=MESH,
        )

    for oi in SEND_ORDER:
        for cc in range(2):
            zz = wrap(z + (1 - 2 * cc) * OFFSETS[oi])
            slot = 3 * (2 * oi + core)
            if oi == len(OFFSETS) - 1:
                src, dst = xs.at[pl.ds(zz + 1, 1)], xbuf.at[pl.ds(slot + 1, 1)]
            else:
                src, dst = xs.at[pl.ds(zz, 3)], xbuf.at[pl.ds(slot, 3)]
            copy(src, dst, 0, dev(zz, cc)).start()
    for n in (1, -1):
        for cc in range(2):
            copy(own_w.at[cc], wbuf.at[2 * (1 - n) + core], 1, dev(z + n, cc)).start()
    copy(own_w.at[1 - core], wbuf.at[2 + core], 1, dev(z, 1 - core)).start()

    wbuf[2 + core] = own_w[core]
    for cc in range(2):
        empty = jnp.zeros(xbuf.shape[1:], BF16)
        xbuf[3 * (10 + cc)] = empty
        xbuf[3 * (10 + cc) + 2] = empty

    for c in loads[5:12]:
        c.wait()
    low_rank = dot(normed, w_dd[...], (((1,), (1,)), ((), ()))).astype(BF16)
    pre = dot(low_rank, w_du[...]) + d_bias[...]
    log_decay = (jnp.minimum(pre, 0.0) - jnp.log1p(jnp.exp(-jnp.abs(pre)))) / TAU
    decay = jnp.exp(log_decay)

    kbs = 8
    tall = kbs * rows
    wide = ep * CAP * kbs
    r_t = lax.rem(iota((tall, rows), 0), rows)
    spread = (r_t == iota((tall, rows), 1)).astype(F32)
    route_rows = dot(
        spread, routes[...].astype(F32), (((1,), (1,)), ((), ())), lax.Precision.HIGHEST
    )
    sc = scores[...]
    e_sc = jnp.exp(sc - jnp.max(sc, axis=0, keepdims=True))
    weights = e_sc / jnp.sum(e_sc, axis=0, keepdims=True)
    weight_rows = dot(spread, weights, (((1,), (1,)), ((), ())), lax.Precision.HIGHEST)
    col = iota((tall, wide), 1)
    row = iota((tall, wide), 0)
    col_e = (col // (CAP * kbs)).astype(F32)
    col_slot = (lax.rem(col, CAP * kbs) // kbs).astype(F32)
    has = jnp.zeros((tall, wide), F32)
    weighted = jnp.zeros((tall, wide), F32)
    for j in range(routes.shape[0]):
        hit = (route_rows[:, j : j + 1] == col_e).astype(F32)
        has += hit
        weighted += hit * weight_rows[:, j : j + 1]
    rr, rc = iota((tall, tall), 0), iota((tall, tall), 1)
    before = (rr // rows == rc // rows) & (rc < rr)
    rank = dot(before.astype(BF16), has.astype(BF16))
    pick = has * (rank == col_slot).astype(F32) * (row // rows == lax.rem(col, kbs)).astype(F32)
    combine = weighted * pick
    combine_hi = combine.astype(BF16)
    combine_lo = (combine - combine_hi.astype(F32)).astype(BF16)
    pick = pick.astype(BF16)

    group = wide // 2
    slots = group // kbs
    p_r, p_c = iota((group, group), 0), iota((group, group), 1)
    perm[...] = (p_c == (lax.rem(p_r, slots) * kbs + p_r // slots)).astype(F32).astype(BF16)
    perm_t[...] = (p_r == (lax.rem(p_c, slots) * kbs + p_c // slots)).astype(F32).astype(BF16)

    loads[12].wait()
    for h in range(HEADS):
        s_h = st[:, h].reshape(rows * DK, DV)
        high = s_h.astype(BF16)
        st_hi[h] = high
        st_lo[h] = (s_h - high.astype(F32)).astype(BF16)

    chunks = 2 * len(OFFSETS)
    units = 3 * (chunks - 2) + 2
    with jax.named_scope("tokens_wait"):
        pltpu.make_async_copy(
            xbuf.at[pl.ds(0, units)], xbuf.at[pl.ds(0, units)], recv_sems.at[0]
        ).wait()
    with jax.named_scope("weights_wait"):
        pltpu.make_async_copy(
            wbuf.at[pl.ds(0, 5)], wbuf.at[pl.ds(0, 5)], recv_sems.at[1]
        ).wait()
    cols = wbuf.shape[2]
    part = None
    for n in range(3):
        x = jnp.concatenate(
            [xbuf[3 * i + n].astype(F32) for i in range(chunks)], axis=0
        ).astype(BF16)
        w = wbuf[2 * n : 2 * n + 2].reshape(2 * wbuf.shape[1], cols)
        p = dot(x, w)
        part = p if part is None else part + p
    for i in range(chunks):
        one = part[rows * i : rows * (i + 1)]
        psend[i] = jnp.concatenate(
            [one[:, : cols // 2], one[:, cols // 2 :]], axis=0
        ).astype(BF16)
    sign = 1 - 2 * core
    for cc in range(2):
        for oi in SEND_ORDER:
            to = dev(z - sign * OFFSETS[oi], cc)
            copy(psend.at[2 * oi + cc], rbuf.at[2 * oi + core], 2, to).start()
    with jax.named_scope("partials_wait"):
        pltpu.make_async_copy(
            psend, rbuf, recv_sems.at[2]
        ).wait()

    sums = []
    for h in range(2):
        total = rbuf[h].astype(F32)
        for oi in range(1, len(OFFSETS)):
            total += rbuf[2 * oi + h].astype(F32)
        sums.append(total)
    queries = sums[0][:rows] * DK ** (-0.5)
    keys = sums[0][rows:]
    values = jnp.concatenate([sums[1][:rows], sums[1][rows:]], axis=1)

    qd = queries * decay
    qk = queries * keys
    block = iota((rows, rows * DK), 1) // DK == iota((rows, rows * DK), 0)
    gain = g_head[...]
    headed = []
    for h in range(HEADS):
        q_h = qd[:, DK * h : DK * (h + 1)]
        lhs = jnp.where(block, jnp.concatenate([q_h] * rows, axis=1), 0.0)
        lhs_hi = lhs.astype(BF16)
        lhs_lo = (lhs - lhs_hi.astype(F32)).astype(BF16)
        both = dot(jnp.concatenate([lhs_hi, lhs_lo], axis=0), st_hi[h])
        a_h = both[:rows] + both[rows:] + dot(lhs_hi, st_lo[h])
        a_h += jnp.sum(qk[:, DK * h : DK * (h + 1)], axis=1, keepdims=True) * values[
            :, DV * h : DV * (h + 1)
        ]
        headed.append(rms(a_h, gain).astype(BF16))
    headed = jnp.concatenate(headed, axis=1)

    loads[13].wait()
    residual = (tok + dot(headed, wo[...])).astype(BF16).astype(F32)
    fed = rms(residual, g_ffn[...])

    lanes = width // kbs
    fed_rows = jnp.concatenate(
        [fed[:, lanes * k : lanes * (k + 1)] for k in range(kbs)], axis=0
    ).astype(BF16)
    dsend[...] = (
        dot(pick, fed_rows, (((0,), (0,)), ((), ()))).astype(BF16).reshape(dsend.shape)
    )

    ring = [o * g for o in range(chips // 2, 0, -1) for g in (1, -1)]
    ring.remove(-(chips // 2))

    def exchange(src, dst, phase, targets):
        for o, cc in targets:
            there = wrap(z + o) * 2 + cc
            copy(src.at[there], dst.at[me], phase, {"ep": there}).start()
        there = 2 * z + 1 - core
        copy(src.at[there], dst.at[me], phase, {"ep": there}).start()
        dst[me] = src[me]

    def arrive(src, dst, phase):
        pltpu.make_async_copy(
            src.at[pl.ds(0, ep - 1)], dst.at[pl.ds(0, ep - 1)], recv_sems.at[phase]
        ).wait()

    with jax.named_scope("dispatch"):
        exchange(dsend, drecv, 3, [(o, cc) for cc in range(2) for o in ring])

    with jax.named_scope("new_state"):
        decay_cols, key_cols = decay.T, keys.T
        for t in range(rows):
            for h in range(HEADS):
                at = slice(DK * h, DK * (h + 1))
                st[t, h] = (
                    decay_cols[at, t : t + 1] * st[t, h]
                    + key_cols[at, t : t + 1] * values[t : t + 1, DV * h : DV * (h + 1)]
                )
        store = pltpu.make_async_copy(st, state_out, load_sems.at[12])
        store.start()

    with jax.named_scope("dispatch_wait"):
        arrive(dsend, drecv, 3)
    with jax.named_scope("expert"):
        some = ep // 2
        for g in range(2):
            came = drecv[some * g : some * (g + 1)].reshape(group, lanes)
            arrived = dot(perm[...], came).astype(BF16)
            for k in range(kbs):
                xin[slots * g : slots * (g + 1), lanes * k : lanes * (k + 1)] = arrived[
                    slots * k : slots * (k + 1)
                ]
        for c in loads[14:]:
            c.wait()
        tile = 256
        for at in range(0, wg.shape[1], tile):
            cols = slice(at, at + tile)
            x = xin[...]
            gate = jnp.minimum(dot(x, wg[:, cols]), LIMIT)
            lin = jnp.clip(dot(x, wl[:, cols]), -LIMIT, LIMIT)
            hid[:, cols] = (gate * jax.nn.sigmoid(ALPHA * gate) * (lin + 1.0)).astype(BF16)
        made = [dot(hid[...], wd[:, lanes * k : lanes * (k + 1)]) for k in range(kbs)]
        for g in range(2):
            expert_out = jnp.concatenate(
                [m[slots * g : slots * (g + 1)] for m in made], axis=0
            ).astype(BF16)
            rsend[some * g : some * (g + 1)] = (
                dot(perm_t[...], expert_out).astype(BF16).reshape(some, CAP * kbs, lanes)
            )
    with jax.named_scope("back"):
        exchange(rsend, rrecv, 4, [(o, cc) for o in ring for cc in range(2)])
    with jax.named_scope("back_wait"):
        arrive(rsend, rrecv, 4)

    back = rrecv[...].reshape(wide, lanes)
    mixed = dot(combine_hi, back) + dot(combine_lo, back)
    for k in range(kbs):
        at = slice(lanes * k, lanes * (k + 1))
        out[:, at] = (residual[:, at] + mixed[rows * k : rows * (k + 1)]).astype(BF16)

    store.wait()
    pltpu.make_async_copy(
        xbuf.at[pl.ds(0, units)], xbuf.at[pl.ds(0, units)], send_sems.at[0]
    ).wait()
    pltpu.make_async_copy(wbuf.at[pl.ds(0, 5)], wbuf.at[pl.ds(0, 5)], send_sems.at[1]).wait()
    pltpu.make_async_copy(psend, rbuf, send_sems.at[2]).wait()
    for src, dst, phase in ((dsend, drecv, 3), (rsend, rrecv, 4)):
        pltpu.make_async_copy(
            src.at[pl.ds(0, ep - 1)], dst.at[pl.ds(0, ep - 1)], send_sems.at[phase]
        ).wait()


def finish(out_in, state_in, out, state_out, out_buf, state_buf, in_sems, out_sems):
    rows = state_in.shape[0]
    ways = [(state_in.at[i], state_buf.at[i], state_out.at[i]) for i in range(rows)]
    ways.append((out_in, out_buf, out))
    ins = [pltpu.make_async_copy(w[0], w[1], in_sems.at[i]) for i, w in enumerate(ways)]
    outs = [pltpu.make_async_copy(w[1], w[2], out_sems.at[i]) for i, w in enumerate(ways)]
    for c in ins:
        c.start()
    for c, d in zip(ins, outs):
        c.wait()
        d.start()
    for d in outs:
        d.wait()


def per_device(
    ep,
    tokens,
    state,
    g_mix,
    w_query,
    w_key,
    w_value,
    w_decay_down,
    w_decay_up,
    decay_bias,
    g_head,
    w_out,
    g_ffn,
    routes,
    route_scores,
    w_gate_in,
    w_lin_in,
    w_down,
):
    rows, width = tokens.shape
    share, qk = w_query.shape
    vw = w_value.shape[1]
    ff = w_gate_in.shape[2]
    lanes = width // 8
    wide = ep * CAP * 8
    vmem = pl.BlockSpec(memory_space=pltpu.VMEM)
    hbm = pl.BlockSpec(memory_space=pltpu.HBM)
    chunks = 2 * len(OFFSETS)
    output, new_state = pl.pallas_call(
        functools.partial(kernel, ep),
        out_shape=(
            jax.ShapeDtypeStruct((rows, width), BF16),
            jax.ShapeDtypeStruct(state.shape, F32),
        ),
        in_specs=[hbm] * 17,
        out_specs=(vmem, hbm),
        scratch_shapes=[
            pltpu.VMEM((rows, width), BF16),
            pltpu.VMEM((1, width), F32),
            pltpu.VMEM(w_decay_down.shape[::-1], BF16),
            pltpu.VMEM(w_decay_up.shape, BF16),
            pltpu.VMEM((1, qk), F32),
            pltpu.VMEM((1, DV), F32),
            pltpu.VMEM((1, width), F32),
            pltpu.VMEM(routes.shape[::-1], jnp.int32),
            pltpu.VMEM(route_scores.shape[::-1], F32),
            pltpu.VMEM((2, share, vw), BF16),
            pltpu.VMEM(state.shape, F32),
            pltpu.VMEM(w_out.shape, BF16),
            pltpu.VMEM(w_gate_in.shape[1:], BF16),
            pltpu.VMEM(w_lin_in.shape[1:], BF16),
            pltpu.VMEM(w_down.shape[1:], BF16),
            pltpu.VMEM((ep // 2 + 2, rows, 2 * share), BF16),
            pltpu.VMEM((3 * chunks, rows, 2 * share), BF16),
            pltpu.VMEM((6, share, vw), BF16),
            pltpu.VMEM((chunks, 2 * rows, vw // 2), BF16),
            pltpu.VMEM((chunks, 2 * rows, vw // 2), BF16),
            pltpu.VMEM((ep, CAP * 8, lanes), BF16),
            pltpu.VMEM((ep, CAP * 8, lanes), BF16),
            pltpu.VMEM((ep, CAP * 8, lanes), BF16),
            pltpu.VMEM((ep, CAP * 8, lanes), BF16),
            pltpu.VMEM((HEADS, rows * DK, DV), BF16),
            pltpu.VMEM((HEADS, rows * DK, DV), BF16),
            pltpu.VMEM((ep * CAP, width), BF16),
            pltpu.VMEM((ep * CAP, ff), BF16),
            pltpu.VMEM((wide // 2, wide // 2), BF16),
            pltpu.VMEM((wide // 2, wide // 2), BF16),
            pltpu.SemaphoreType.DMA((17,)),
            pltpu.SemaphoreType.DMA((5,)),
            pltpu.SemaphoreType.DMA((5,)),
        ],
        compiler_params=pltpu.CompilerParams(
            collective_id=0, has_side_effects=True, vmem_limit_bytes=63_000_000
        ),
        name="layer",
    )(
        tokens,
        g_mix.reshape(1, width),
        w_decay_down.T,
        w_decay_up,
        decay_bias.reshape(1, qk),
        g_head.reshape(1, DV),
        g_ffn.reshape(1, width),
        routes.T,
        route_scores.T,
        state,
        w_query,
        w_key,
        w_value,
        w_out,
        w_gate_in,
        w_lin_in,
        w_down,
    )
    return pl.pallas_call(
        finish,
        out_shape=(
            jax.ShapeDtypeStruct((rows, width), BF16),
            jax.ShapeDtypeStruct(state.shape, F32),
        ),
        in_specs=[hbm] * 2,
        out_specs=(hbm, hbm),
        scratch_shapes=[
            pltpu.VMEM((rows, width), BF16),
            pltpu.VMEM(state.shape, F32),
            pltpu.SemaphoreType.DMA((rows + 1,)),
            pltpu.SemaphoreType.DMA((rows + 1,)),
        ],
        compiler_params=pltpu.CompilerParams(vmem_limit_bytes=63_000_000),
        name="finish",
    )(output, new_state)


def solution(mesh):
    shard = P(("grp", "ep"), None)
    experts = P("ep", None, None)
    return jax.shard_map(
        functools.partial(per_device, mesh.shape["ep"]),
        mesh=mesh,
        in_specs=(
            shard,
            P(("grp", "ep"), None, None, None),
            P(),
            P("ep", None),
            P("ep", None),
            P("ep", None),
            P(),
            P(),
            P(),
            P(),
            P(),
            P(),
            shard,
            shard,
            experts,
            experts,
            experts,
        ),
        out_specs=(shard, P(("grp", "ep"), None, None, None)),
        check_vma=False,
    )
```

```python
import functools

import jax
import jax.numpy as jnp
from jax import lax
from jax.experimental import pallas as pl
from jax.experimental.pallas import tpu as pltpu
from jax.sharding import PartitionSpec as P

MESH = pl.DeviceIdType.MESH
F32 = jnp.float32
BF16 = jnp.bfloat16

HEADS = 8
DK = 64
DV = 128
CAP = 2
EPS = 1e-06
TAU = 16.0
ALPHA = 1.702
LIMIT = 7.0

OFFSETS = (1, 4, 7, -2, -5, -7)
SEND_ORDER = (2, 5, 4, 1, 3, 0)


def rms(values, gain):
    return values * lax.rsqrt(jnp.mean(values * values, axis=-1, keepdims=True) + EPS) * gain


def dot(a, b, dims=None, precision=None):
    dims = dims or (((1,), (0,)), ((), ()))
    return lax.dot_general(a, b, dims, precision=precision, preferred_element_type=F32)


def iota(shape, dim):
    return lax.broadcasted_iota(jnp.int32, shape, dim)


def kernel(
    ep,
    tokens_in,
    g_mix_in,
    w_dd_in,
    w_du_in,
    d_bias_in,
    g_head_in,
    g_ffn_in,
    routes_in,
    scores_in,
    state,
    w_q,
    w_k,
    w_v,
    w_out,
    w_gate,
    w_lin,
    w_down,
    out,
    state_out,
    tokens,
    g_mix,
    w_dd,
    w_du,
    d_bias,
    g_head,
    g_ffn,
    routes,
    scores,
    own_w,
    st,
    wo,
    wg,
    wl,
    wd,
    xs,
    xbuf,
    wbuf,
    psend,
    rbuf,
    dsend,
    drecv,
    rsend,
    rrecv,
    st_hi,
    st_lo,
    xin,
    hid,
    perm,
    perm_t,
    load_sems,
    send_sems,
    recv_sems,
):
    rows, width = tokens.shape
    chips = ep // 2
    me = lax.axis_index("ep")
    z, core = me // 2, lax.rem(me, 2)

    def wrap(i):
        return lax.rem(i + 2 * chips, chips)

    def dev(zz, cc):
        return {"ep": wrap(zz) * 2 + cc}

    half = w_q.shape[1]
    pairs = [
        (tokens_in, tokens),
        (g_mix_in, g_mix),
        (w_q, own_w.at[0, :, pl.ds(0, half)]),
        (w_k, own_w.at[0, :, pl.ds(half, half)]),
        (w_v, own_w.at[1]),
        (w_dd_in, w_dd),
        (w_du_in, w_du),
        (d_bias_in, d_bias),
        (routes_in, routes),
        (scores_in, scores),
        (g_head_in, g_head),
        (g_ffn_in, g_ffn),
        (state, st),
        (w_out, wo),
        (w_gate.at[0], wg),
        (w_lin.at[0], wl),
        (w_down.at[0], wd),
    ]
    loads = [
        pltpu.make_async_copy(src, dst, load_sems.at[i]) for i, (src, dst) in enumerate(pairs)
    ]
    barrier = pltpu.get_barrier_semaphore()

    hops = sorted({abs(o) for o in OFFSETS}, reverse=True)
    peers = [dev(z + o * g, c) for o in hops for g in (1, -1) for c in range(2)]
    peers.append(dev(z, 1 - core))

    with jax.named_scope("hello"):
        for to in peers:
            pl.semaphore_signal(barrier, inc=1, device_id=to, device_id_type=MESH)
        for c in loads:
            c.start()
        for c in loads[:2]:
            c.wait()

    tok = tokens[...].astype(F32)
    normed = rms(tok, g_mix[...]).astype(BF16)
    for i in range(chips + 2):
        j = (i - 1) % chips
        xs[i] = normed[:, 128 * j : 128 * (j + 1)]

    for c in loads[2:5]:
        c.wait()

    with jax.named_scope("barrier"):
        pl.semaphore_wait(barrier, len(peers))

    def copy(src, dst, phase, device):
        return pltpu.make_async_remote_copy(
            src_ref=src,
            dst_ref=dst,
            send_sem=send_sems.at[phase],
            recv_sem=recv_sems.at[phase],
            device_id=device,
            device_id_type=MESH,
        )

    for oi in SEND_ORDER:
        for cc in range(2):
            zz = wrap(z + (1 - 2 * cc) * OFFSETS[oi])
            slot = 3 * (2 * oi + core)
            if oi == len(OFFSETS) - 1:
                src, dst = xs.at[pl.ds(zz + 1, 1)], xbuf.at[pl.ds(slot + 1, 1)]
            else:
                src, dst = xs.at[pl.ds(zz, 3)], xbuf.at[pl.ds(slot, 3)]
            copy(src, dst, 0, dev(zz, cc)).start()
    for n in (1, -1):
        for cc in range(2):
            copy(own_w.at[cc], wbuf.at[2 * (1 - n) + core], 1, dev(z + n, cc)).start()
    copy(own_w.at[1 - core], wbuf.at[2 + core], 5, dev(z, 1 - core)).start()

    wbuf[2 + core] = own_w[core]
    for cc in range(2):
        empty = jnp.zeros(xbuf.shape[1:], BF16)
        xbuf[3 * (10 + cc)] = empty
        xbuf[3 * (10 + cc) + 2] = empty

    for c in loads[5:12]:
        c.wait()
    low_rank = dot(normed, w_dd[...], (((1,), (1,)), ((), ()))).astype(BF16)
    pre = dot(low_rank, w_du[...]) + d_bias[...]
    log_decay = (jnp.minimum(pre, 0.0) - jnp.log1p(jnp.exp(-jnp.abs(pre)))) / TAU
    decay = jnp.exp(log_decay)

    kbs = 8
    tall = kbs * rows
    wide = ep * CAP * kbs
    r_t = lax.rem(iota((tall, rows), 0), rows)
    spread = (r_t == iota((tall, rows), 1)).astype(F32)
    route_rows = dot(
        spread, routes[...].astype(F32), (((1,), (1,)), ((), ())), lax.Precision.HIGHEST
    )
    sc = scores[...]
    e_sc = jnp.exp(sc - jnp.max(sc, axis=0, keepdims=True))
    weights = e_sc / jnp.sum(e_sc, axis=0, keepdims=True)
    weight_rows = dot(spread, weights, (((1,), (1,)), ((), ())), lax.Precision.HIGHEST)
    col = iota((tall, wide), 1)
    row = iota((tall, wide), 0)
    col_e = (col // (CAP * kbs)).astype(F32)
    col_slot = (lax.rem(col, CAP * kbs) // kbs).astype(F32)
    has = jnp.zeros((tall, wide), F32)
    weighted = jnp.zeros((tall, wide), F32)
    for j in range(routes.shape[0]):
        hit = (route_rows[:, j : j + 1] == col_e).astype(F32)
        has += hit
        weighted += hit * weight_rows[:, j : j + 1]
    rr, rc = iota((tall, tall), 0), iota((tall, tall), 1)
    before = (rr // rows == rc // rows) & (rc < rr)
    rank = dot(before.astype(BF16), has.astype(BF16))
    pick = has * (rank == col_slot).astype(F32) * (row // rows == lax.rem(col, kbs)).astype(F32)
    combine = weighted * pick
    combine_hi = combine.astype(BF16)
    combine_lo = (combine - combine_hi.astype(F32)).astype(BF16)
    pick = pick.astype(BF16)

    group = wide // 2
    slots = group // kbs
    p_r, p_c = iota((group, group), 0), iota((group, group), 1)
    perm[...] = (p_c == (lax.rem(p_r, slots) * kbs + p_r // slots)).astype(F32).astype(BF16)
    perm_t[...] = (p_r == (lax.rem(p_c, slots) * kbs + p_c // slots)).astype(F32).astype(BF16)

    loads[12].wait()
    for h in range(HEADS):
        s_h = st[:, h].reshape(rows * DK, DV)
        high = s_h.astype(BF16)
        st_hi[h] = high
        st_lo[h] = (s_h - high.astype(F32)).astype(BF16)

    chunks = 2 * len(OFFSETS)
    units = 3 * (chunks - 2) + 2
    with jax.named_scope("tokens_wait"):
        pltpu.make_async_copy(
            xbuf.at[pl.ds(0, units)], xbuf.at[pl.ds(0, units)], recv_sems.at[0]
        ).wait()
    pltpu.make_async_copy(wbuf.at[0], wbuf.at[0], recv_sems.at[5]).wait()
    cols = wbuf.shape[2]
    part = None
    for n in (1, 0, 2):
        if n == 0:
            with jax.named_scope("weights_wait"):
                pltpu.make_async_copy(
                    wbuf.at[pl.ds(0, 4)], wbuf.at[pl.ds(0, 4)], recv_sems.at[1]
                ).wait()
        x = jnp.concatenate(
            [xbuf[3 * i + n].astype(F32) for i in range(chunks)], axis=0
        ).astype(BF16)
        w = wbuf[2 * n : 2 * n + 2].reshape(2 * wbuf.shape[1], cols)
        p = dot(x, w)
        part = p if part is None else part + p
    for i in range(chunks):
        one = part[rows * i : rows * (i + 1)]
        psend[i] = jnp.concatenate(
            [one[:, : cols // 2], one[:, cols // 2 :]], axis=0
        ).astype(BF16)
    sign = 1 - 2 * core
    for cc in range(2):
        for oi in SEND_ORDER:
            to = dev(z - sign * OFFSETS[oi], cc)
            copy(psend.at[2 * oi + cc], rbuf.at[2 * oi + core], 2, to).start()
    with jax.named_scope("partials_wait"):
        pltpu.make_async_copy(
            psend, rbuf, recv_sems.at[2]
        ).wait()

    sums = []
    for h in range(2):
        total = rbuf[h].astype(F32)
        for oi in range(1, len(OFFSETS)):
            total += rbuf[2 * oi + h].astype(F32)
        sums.append(total)
    queries = sums[0][:rows] * DK ** (-0.5)
    keys = sums[0][rows:]
    values = jnp.concatenate([sums[1][:rows], sums[1][rows:]], axis=1)

    qd = queries * decay
    qk = queries * keys
    block = iota((rows, rows * DK), 1) // DK == iota((rows, rows * DK), 0)
    gain = g_head[...]
    headed = []
    for h in range(HEADS):
        q_h = qd[:, DK * h : DK * (h + 1)]
        lhs = jnp.where(block, jnp.concatenate([q_h] * rows, axis=1), 0.0)
        lhs_hi = lhs.astype(BF16)
        lhs_lo = (lhs - lhs_hi.astype(F32)).astype(BF16)
        both = dot(jnp.concatenate([lhs_hi, lhs_lo], axis=0), st_hi[h])
        a_h = both[:rows] + both[rows:] + dot(lhs_hi, st_lo[h])
        a_h += jnp.sum(qk[:, DK * h : DK * (h + 1)], axis=1, keepdims=True) * values[
            :, DV * h : DV * (h + 1)
        ]
        headed.append(rms(a_h, gain).astype(BF16))
    headed = jnp.concatenate(headed, axis=1)

    loads[13].wait()
    residual = (tok + dot(headed, wo[...])).astype(BF16).astype(F32)
    fed = rms(residual, g_ffn[...])

    lanes = width // kbs
    fed_rows = jnp.concatenate(
        [fed[:, lanes * k : lanes * (k + 1)] for k in range(kbs)], axis=0
    ).astype(BF16)
    dsend[...] = (
        dot(pick, fed_rows, (((0,), (0,)), ((), ()))).astype(BF16).reshape(dsend.shape)
    )

    ring = [o * g for o in range(chips // 2, 0, -1) for g in (1, -1)]
    ring.remove(-(chips // 2))

    def exchange(src, dst, phase, targets):
        for o, cc in targets:
            there = wrap(z + o) * 2 + cc
            copy(src.at[there], dst.at[me], phase, {"ep": there}).start()
        there = 2 * z + 1 - core
        copy(src.at[there], dst.at[me], phase, {"ep": there}).start()
        dst[me] = src[me]

    def arrive(src, dst, phase):
        pltpu.make_async_copy(
            src.at[pl.ds(0, ep - 1)], dst.at[pl.ds(0, ep - 1)], recv_sems.at[phase]
        ).wait()

    with jax.named_scope("dispatch"):
        exchange(dsend, drecv, 3, [(o, cc) for cc in range(2) for o in ring])

    with jax.named_scope("new_state"):
        decay_cols, key_cols = decay.T, keys.T
        for t in range(rows):
            for h in range(HEADS):
                at = slice(DK * h, DK * (h + 1))
                st[t, h] = (
                    decay_cols[at, t : t + 1] * st[t, h]
                    + key_cols[at, t : t + 1] * values[t : t + 1, DV * h : DV * (h + 1)]
                )
        store = pltpu.make_async_copy(st, state_out, load_sems.at[12])
        store.start()

    with jax.named_scope("dispatch_wait"):
        arrive(dsend, drecv, 3)
    with jax.named_scope("expert"):
        some = ep // 2
        for g in range(2):
            came = drecv[some * g : some * (g + 1)].reshape(group, lanes)
            arrived = dot(perm[...], came).astype(BF16)
            for k in range(kbs):
                xin[slots * g : slots * (g + 1), lanes * k : lanes * (k + 1)] = arrived[
                    slots * k : slots * (k + 1)
                ]
        for c in loads[14:]:
            c.wait()
        tile = 256
        for at in range(0, wg.shape[1], tile):
            cols = slice(at, at + tile)
            x = xin[...]
            gate = jnp.minimum(dot(x, wg[:, cols]), LIMIT)
            lin = jnp.clip(dot(x, wl[:, cols]), -LIMIT, LIMIT)
            hid[:, cols] = (gate * jax.nn.sigmoid(ALPHA * gate) * (lin + 1.0)).astype(BF16)
        made = [dot(hid[...], wd[:, lanes * k : lanes * (k + 1)]) for k in range(kbs)]
        for g in range(2):
            expert_out = jnp.concatenate(
                [m[slots * g : slots * (g + 1)] for m in made], axis=0
            ).astype(BF16)
            rsend[some * g : some * (g + 1)] = (
                dot(perm_t[...], expert_out).astype(BF16).reshape(some, CAP * kbs, lanes)
            )
    with jax.named_scope("back"):
        exchange(rsend, rrecv, 4, [(o, cc) for o in ring for cc in range(2)])
    with jax.named_scope("back_wait"):
        arrive(rsend, rrecv, 4)

    back = rrecv[...].reshape(wide, lanes)
    both = dot(jnp.concatenate([combine_hi, combine_lo], axis=0), back)
    mixed = both[:tall] + both[tall:]
    for k in range(kbs):
        at = slice(lanes * k, lanes * (k + 1))
        out[:, at] = (residual[:, at] + mixed[rows * k : rows * (k + 1)]).astype(BF16)

    store.wait()
    pltpu.make_async_copy(
        xbuf.at[pl.ds(0, units)], xbuf.at[pl.ds(0, units)], send_sems.at[0]
    ).wait()
    pltpu.make_async_copy(wbuf.at[pl.ds(0, 4)], wbuf.at[pl.ds(0, 4)], send_sems.at[1]).wait()
    pltpu.make_async_copy(wbuf.at[0], wbuf.at[0], send_sems.at[5]).wait()
    pltpu.make_async_copy(psend, rbuf, send_sems.at[2]).wait()
    for src, dst, phase in ((dsend, drecv, 3), (rsend, rrecv, 4)):
        pltpu.make_async_copy(
            src.at[pl.ds(0, ep - 1)], dst.at[pl.ds(0, ep - 1)], send_sems.at[phase]
        ).wait()


def finish(out_in, state_in, out, state_out, out_buf, state_buf, in_sems, out_sems):
    rows = state_in.shape[0]
    ways = [(state_in.at[i], state_buf.at[i], state_out.at[i]) for i in range(rows)]
    ways.append((out_in, out_buf, out))
    ins = [pltpu.make_async_copy(w[0], w[1], in_sems.at[i]) for i, w in enumerate(ways)]
    outs = [pltpu.make_async_copy(w[1], w[2], out_sems.at[i]) for i, w in enumerate(ways)]
    for c in ins:
        c.start()
    for c, d in zip(ins, outs):
        c.wait()
        d.start()
    for d in outs:
        d.wait()


def per_device(
    ep,
    tokens,
    state,
    g_mix,
    w_query,
    w_key,
    w_value,
    w_decay_down,
    w_decay_up,
    decay_bias,
    g_head,
    w_out,
    g_ffn,
    routes,
    route_scores,
    w_gate_in,
    w_lin_in,
    w_down,
):
    rows, width = tokens.shape
    share, qk = w_query.shape
    vw = w_value.shape[1]
    ff = w_gate_in.shape[2]
    lanes = width // 8
    wide = ep * CAP * 8
    vmem = pl.BlockSpec(memory_space=pltpu.VMEM)
    hbm = pl.BlockSpec(memory_space=pltpu.HBM)
    chunks = 2 * len(OFFSETS)
    output, new_state = pl.pallas_call(
        functools.partial(kernel, ep),
        out_shape=(
            jax.ShapeDtypeStruct((rows, width), BF16),
            jax.ShapeDtypeStruct(state.shape, F32),
        ),
        in_specs=[hbm] * 17,
        out_specs=(vmem, hbm),
        scratch_shapes=[
            pltpu.VMEM((rows, width), BF16),
            pltpu.VMEM((1, width), F32),
            pltpu.VMEM(w_decay_down.shape[::-1], BF16),
            pltpu.VMEM(w_decay_up.shape, BF16),
            pltpu.VMEM((1, qk), F32),
            pltpu.VMEM((1, DV), F32),
            pltpu.VMEM((1, width), F32),
            pltpu.VMEM(routes.shape[::-1], jnp.int32),
            pltpu.VMEM(route_scores.shape[::-1], F32),
            pltpu.VMEM((2, share, vw), BF16),
            pltpu.VMEM(state.shape, F32),
            pltpu.VMEM(w_out.shape, BF16),
            pltpu.VMEM(w_gate_in.shape[1:], BF16),
            pltpu.VMEM(w_lin_in.shape[1:], BF16),
            pltpu.VMEM(w_down.shape[1:], BF16),
            pltpu.VMEM((ep // 2 + 2, rows, 2 * share), BF16),
            pltpu.VMEM((3 * chunks, rows, 2 * share), BF16),
            pltpu.VMEM((6, share, vw), BF16),
            pltpu.VMEM((chunks, 2 * rows, vw // 2), BF16),
            pltpu.VMEM((chunks, 2 * rows, vw // 2), BF16),
            pltpu.VMEM((ep, CAP * 8, lanes), BF16),
            pltpu.VMEM((ep, CAP * 8, lanes), BF16),
            pltpu.VMEM((ep, CAP * 8, lanes), BF16),
            pltpu.VMEM((ep, CAP * 8, lanes), BF16),
            pltpu.VMEM((HEADS, rows * DK, DV), BF16),
            pltpu.VMEM((HEADS, rows * DK, DV), BF16),
            pltpu.VMEM((ep * CAP, width), BF16),
            pltpu.VMEM((ep * CAP, ff), BF16),
            pltpu.VMEM((wide // 2, wide // 2), BF16),
            pltpu.VMEM((wide // 2, wide // 2), BF16),
            pltpu.SemaphoreType.DMA((17,)),
            pltpu.SemaphoreType.DMA((6,)),
            pltpu.SemaphoreType.DMA((6,)),
        ],
        compiler_params=pltpu.CompilerParams(
            collective_id=0, has_side_effects=True, vmem_limit_bytes=63_000_000
        ),
        name="layer",
    )(
        tokens,
        g_mix.reshape(1, width),
        w_decay_down.T,
        w_decay_up,
        decay_bias.reshape(1, qk),
        g_head.reshape(1, DV),
        g_ffn.reshape(1, width),
        routes.T,
        route_scores.T,
        state,
        w_query,
        w_key,
        w_value,
        w_out,
        w_gate_in,
        w_lin_in,
        w_down,
    )
    return pl.pallas_call(
        finish,
        out_shape=(
            jax.ShapeDtypeStruct((rows, width), BF16),
            jax.ShapeDtypeStruct(state.shape, F32),
        ),
        in_specs=[hbm] * 2,
        out_specs=(hbm, hbm),
        scratch_shapes=[
            pltpu.VMEM((rows, width), BF16),
            pltpu.VMEM(state.shape, F32),
            pltpu.SemaphoreType.DMA((rows + 1,)),
            pltpu.SemaphoreType.DMA((rows + 1,)),
        ],
        compiler_params=pltpu.CompilerParams(vmem_limit_bytes=63_000_000),
        name="finish",
    )(output, new_state)


def solution(mesh):
    shard = P(("grp", "ep"), None)
    experts = P("ep", None, None)
    return jax.shard_map(
        functools.partial(per_device, mesh.shape["ep"]),
        mesh=mesh,
        in_specs=(
            shard,
            P(("grp", "ep"), None, None, None),
            P(),
            P("ep", None),
            P("ep", None),
            P("ep", None),
            P(),
            P(),
            P(),
            P(),
            P(),
            P(),
            shard,
            shard,
            experts,
            experts,
            experts,
        ),
        out_specs=(shard, P(("grp", "ep"), None, None, None)),
        check_vma=False,
    )
```
